256 devices in a mesh: gr: 2 (over z_hi), sp: 16 (over z_lo, y), tp: 8 (over x, core).
Axes of the slice: x: 4, y: 4, z: 8 (z_hi: 2, z_lo: 4; z = z_hi * 4 + z_lo), core: 2. Of those that a mesh axis runs over, the one named last changes fastest.
Arguments:
- tokens: bfloat16 [8, 8, 2048, 4096], P('gr', 'tp', 'sp'), may hold values from -6 to 6
- ln_gain: bfloat16 [4096], replicated, may hold values from 0.099609375 to 1.8984375
- w_key: bfloat16 [4096, 256], P('sp'), may hold values from -0.09375 to 0.09375
- w_value: bfloat16 [4096, 256], P('sp'), may hold values from -0.09375 to 0.09375
- queries: bfloat16 [32, 512], P(('gr', 'sp')), may hold values from -6 to 6
- head_shift: float32 [4, 8], replicated
- key_shift: float32 [32, 16384], P(('gr', 'sp'), 'tp')
Outputs:
- kv_cache: bfloat16 [32, 16384, 128], P(('gr', 'sp'), 'tp')
- first_read: float32 [32, 512], P(('gr', 'sp'))
The draws below stay inside these ranges and needn't reach their ends.
All inputs are finite; a program needn't handle non-finite values.
Results may differ from the reference program's by a relative error of at most 0.0064.
Values may be sent and summed in bfloat16 or wider, within the bound.
A program may use at most 64 MiB of HBM per device.

```python
import math
import jax
import jax.numpy as jnp
from jax import lax

D = 4096
HD = 64
KVH = 4
GROUP = 8
SEQS = 8
SECTIONS = 8
SPAN = 2048
LEN = 16384
PAIRS = 32


def draw_head_shift(key, part):
    first, second, third = jax.random.split(key, 3)
    fast_share = 0.5
    picker = jax.random.uniform(first, (KVH, GROUP), jnp.float32)
    fast_value = jax.random.uniform(second, (KVH, GROUP), jnp.float32, -4.5, -3.5)
    slow_value = -math.log(LEN) - 1.5 + jax.random.uniform(third, (KVH, GROUP), jnp.float32, -0.3, 0.3)
    return jnp.where(picker < fast_share, fast_value, slow_value)


def draw_key_shift(key, part):
    first, second, third, fourth = jax.random.split(key, 4)
    spread = 0.7
    section_level = jax.random.uniform(first, (PAIRS, SECTIONS), jnp.float32, -spread, spread)
    section_full = jnp.repeat(section_level, SPAN, axis=1)
    rough = jax.random.uniform(second, (PAIRS, LEN), jnp.float32, -0.5, 0.5)
    places = jax.random.randint(third, (PAIRS, 4), 0, LEN)
    marks = jnp.any(jnp.arange(LEN)[None, None, :] == places[:, :, None], axis=1)
    height = math.log(LEN) + 0.5 + jax.random.uniform(fourth, (PAIRS, LEN), jnp.float32, -0.3, 0.3)
    return section_full + rough + jnp.where(marks, height, 0.0)


def levels(key, extent, cuts, smallest, top_value):
    level = 1.0
    for dim, blocks in cuts:
        heights = jax.random.uniform(jax.random.fold_in(jax.random.fold_in(key, 6), dim), (blocks,), jnp.float32, smallest / len(cuts), top_value / len(cuts))
        level = level * jnp.repeat(jnp.exp(heights), extent[dim] // blocks).reshape((-1,) + (1,) * (len(extent) - 1 - dim))
    return level


def bell_draw(rng, shape, deviation, most, cuts=(), kind=jnp.bfloat16):
    values = jax.random.normal(rng, shape, jnp.float32) * deviation
    if len(cuts) > 0:
        values = levels(rng, shape, cuts, -0.22, 0.18) * values
    return jnp.clip(values, min=-most, max=most).astype(kind)


def setup_inputs(seed: int = 0) -> dict:
    splits = jax.random.split(jax.random.key(seed), 8)
    tokens = bell_draw(splits[0], (SEQS, SECTIONS, SPAN, D), 1.0, 6.0, ((0, 2), (1, 8), (2, 16)))
    ln_gain = jnp.clip(1.0 + 0.18 * jax.random.normal(splits[1], (D,), jnp.float32), 0.099609375, 1.8984375).astype(jnp.bfloat16)
    w_key = bell_draw(splits[2], (D, KVH * HD), D ** -0.5, 0.09375, ((0, 16),))
    w_value = bell_draw(splits[3], (D, KVH * HD), D ** -0.5, 0.09375, ((0, 16),))
    queries = bell_draw(splits[4], (PAIRS, GROUP * HD), 1.0, 6.0, ((0, 32),))
    head_shift = draw_head_shift(jax.random.fold_in(splits[7], 71), 0)
    key_shift = draw_key_shift(jax.random.fold_in(splits[7], 71), 0)
    return {"tokens": tokens, "ln_gain": ln_gain, "w_key": w_key, "w_value": w_value, "queries": queries, "head_shift": head_shift, "key_shift": key_shift}


epsilon = 1e-05

def project_sequence(block, ln_gain, w_key, w_value):
    flat_rows = block.reshape(LEN, D).astype(jnp.float32)
    row_mean = lax.optimization_barrier(jnp.mean(flat_rows, axis=1, keepdims=True))
    centred = flat_rows - row_mean
    row_var = lax.optimization_barrier(jnp.mean(centred * centred, axis=1, keepdims=True))
    normed = (centred * lax.rsqrt(row_var + epsilon) * ln_gain.astype(jnp.float32)).astype(jnp.bfloat16)
    keys = jnp.dot(normed, w_key, preferred_element_type=jnp.float32).astype(jnp.bfloat16)
    values = jnp.dot(normed, w_value, preferred_element_type=jnp.float32).astype(jnp.bfloat16)
    joined = jnp.concatenate([keys.reshape(LEN, KVH, HD), values.reshape(LEN, KVH, HD)], axis=2)
    return jnp.transpose(joined, (1, 0, 2))

def read_pair(pair_cache, query, shift_row, head_row):
    keys = pair_cache[:, :HD]
    values = pair_cache[:, HD:]
    logits = jnp.dot(query.reshape(GROUP, HD), keys.T, preferred_element_type=jnp.float32) * HD ** (-0.5)
    logits = logits + head_row[:, None] + shift_row[None, :]
    log_beta = jax.nn.log_sigmoid(logits)
    log_keep = (log_beta - logits).reshape(GROUP, SECTIONS, SPAN)
    within = lax.cumsum(log_keep, axis=2, reverse=True) - log_keep
    local_weight = jnp.exp(log_beta.reshape(GROUP, SECTIONS, SPAN) + within).astype(jnp.bfloat16)
    parts = jnp.einsum('gsj,sjd->gsd', local_weight.astype(jnp.float32), values.reshape(SECTIONS, SPAN, HD).astype(jnp.float32))
    totals = lax.optimization_barrier(jnp.sum(log_keep, axis=2))
    carry = lax.cumsum(totals, axis=1, reverse=True) - totals
    return lax.optimization_barrier(jnp.sum(jnp.exp(carry)[:, :, None] * parts, axis=1)).reshape(GROUP * HD)

def reference(tokens, ln_gain, w_key, w_value, queries, head_shift, key_shift):
    caches = lax.map(lambda block: project_sequence(block, ln_gain, w_key, w_value), tokens)
    kv_cache = caches.reshape(PAIRS, LEN, 2 * HD)
    head_rows = jnp.tile(head_shift, (SEQS, 1))
    first_read = lax.map(lambda items: read_pair(items[0], items[1], items[2], items[3]), (kv_cache, queries, key_shift, head_rows))
    return (kv_cache, first_read)
```

```python
import functools

import jax
import jax.numpy as jnp
from jax import lax
from jax.experimental import pallas as pl
from jax.experimental.pallas import tpu as pltpu
from jax.sharding import PartitionSpec as P

MESH = pl.DeviceIdType.MESH
F32, BF16 = jnp.float32, jnp.bfloat16
D, HD, KVH, GROUP = 4096, 64, 4, 8
EPS = 1e-05
SPLIT = ((128, 128, 0), (0, 0, 256))
MAX_COPIES = 112


def kernel(
    tok_hbm, gain_hbm, wk_hbm, wv_hbm, q_hbm, hs_hbm, ks_hbm,
    cache_hbm, read_hbm,
    tok, nrm, w, acc, kvs, kvr, cache, gain, qv, hsv, ksv, rdv, xs, xr,
    local_sem, send_sem, recv_sem,
):
    gr, sp, tp = lax.axis_index("gr"), lax.axis_index("sp"), lax.axis_index("tp")
    x, core = tp // 2, tp % 2
    zl, y = sp // 4, sp % 4
    z = gr * 4 + zl

    def at_z(k):
        far = (z + k) % 8
        return (far // 4, (far % 4) * 4 + y, tp)

    def at_y(k):
        return (gr, zl * 4 + (y + k) % 4, tp)

    def at_x(k):
        return (gr, sp, ((x + k) % 4) * 2 + core)

    def at_sp(k):
        return (gr, (sp + k) % 16, tp)

    def at_tp(k):
        return (gr, sp, (tp + k) % 8)

    sibling = (gr, sp, x * 2 + 1 - core)

    copies = []

    def send(src, dst, device):
        number = len(copies)
        copy = pltpu.make_async_remote_copy(
            src_ref=src,
            dst_ref=dst,
            send_sem=send_sem.at[number],
            recv_sem=recv_sem.at[number],
            device_id=device,
            device_id_type=MESH,
        )
        copy.start()
        copies.append(copy)
        return copy

    locals_ = []

    def fetch(src, dst):
        copy = pltpu.make_async_copy(src, dst, local_sem.at[len(locals_)])
        copy.start()
        locals_.append(copy)
        return copy

    plan = []
    for c in range(2):
        a, b, d = SPLIT[c]
        p = {"c": c, "a": a // 2, "b": b // 2, "d": d // 8}
        p["a0"] = pl.multiple_of(core * (a // 2), 32)
        p["b0"] = pl.multiple_of(a + core * (b // 2), 32)
        p["d0"] = pl.multiple_of(a + b + tp * (d // 8), 16)
        p["own"] = []
        for size in ("a", "b", "d"):
            if p[size]:
                rows = pl.ds(p[size + "0"], p[size])
                source = (wk_hbm, wv_hbm)[c].at[rows, :]
                p["own"].append(fetch(source, w.at[c, zl, y, rows, :]))
        plan.append(p)
    got_gain = fetch(gain_hbm, gain)
    got_tok = [fetch(tok_hbm.at[s, 0], tok.at[s]) for s in range(4)]
    got_small = [fetch(q_hbm, qv), fetch(hs_hbm, hsv), fetch(ks_hbm, ksv)]

    barrier = pltpu.get_barrier_semaphore()
    friends = [at_z(k) for k in (1, -1, 2, -2)]
    friends += [at_sp(k) for k in range(1, 16)]
    friends += [at_tp(k) for k in range(1, 8)]
    for friend in friends:
        pl.semaphore_signal(barrier, inc=1, device_id=friend, device_id_type=MESH)
    pl.semaphore_wait(barrier, len(friends))

    def piece(c, zi, yi, start, count):
        return w.at[c, zi, yi, pl.ds(start, count), :]

    def both(c, zi, yi, start, count, device):
        ref = piece(c, zi, yi, start, count)
        return send(ref, ref, device)

    every = pl.ds(0, 4)
    low, high = pl.ds(0, 2), pl.ds(2, 2)

    def stage1(p):
        c = p["c"]
        p["s1"] = []
        if p["a"]:
            for k in (1, -1, 2 - 4 * core):
                p["s1"].append(both(c, zl, y, p["a0"], p["a"], at_z(k)))
        if p["b"]:
            for k in (1, -1, 2):
                p["s1"].append(both(c, zl, y, p["b0"], p["b"], at_y(k)))
        if p["d"]:
            for k in range(1, 16):
                p["s1"].append(both(c, zl, y, p["d0"], p["d"], at_sp(k)))

    def stage2(p):
        c = p["c"]
        for copy in p["s1"]:
            copy.wait_recv()
        p["s2"], p["pair"] = [], []
        if p["a"]:
            for k in (1, -1):
                p["s2"].append(both(c, every, y, p["a0"], p["a"], at_y(k)))
        if p["b"]:
            for k in (1, -1):
                p["s2"].append(both(c, zl, every, p["b0"], p["b"], at_z(k)))
        if p["d"]:
            for k in (1, -1):
                p["s2"].append(both(c, every, every, p["d0"], p["d"], at_x(k)))
        if p["a"]:
            p["pair"].append(both(c, every, y, p["a0"], p["a"], sibling))
        if p["b"]:
            p["pair"].append(both(c, zl, every, p["b0"], p["b"], sibling))
        if p["d"]:
            p["pair"].append(both(c, every, every, p["d0"], p["d"], sibling))

    def stage3(p):
        c = p["c"]
        for copy in p["s2"]:
            copy.wait_recv()
        p["s3"] = []
        up, down = (y + 1) % 4, (y + 3) % 4
        zup, zdown = (zl + 1) % 4, (zl + 3) % 4
        xup, xdown = (x + 1) % 4, (x + 3) % 4
        if p["a"]:
            p["s3"].append(both(c, low, down, p["a0"], p["a"], at_y(1)))
            p["s3"].append(both(c, high, up, p["a0"], p["a"], at_y(-1)))
        if p["b"]:
            p["s3"].append(both(c, zdown, low, p["b0"], p["b"], at_z(1)))
            p["s3"].append(both(c, zup, high, p["b0"], p["b"], at_z(-1)))
        if p["d"]:
            base = p["d0"] - tp * p["d"]
            first = pl.multiple_of(base + (xdown * 2 + core) * p["d"], 16)
            second = pl.multiple_of(base + (xup * 2 + core) * p["d"], 16)
            p["s3"].append(both(c, low, every, first, p["d"], at_x(1)))
            p["s3"].append(both(c, high, every, second, p["d"], at_x(-1)))
        if p["a"]:
            for side in (down, up):
                p["pair"].append(both(c, every, side, p["a0"], p["a"], sibling))
        if p["b"]:
            for side in (zdown, zup):
                p["pair"].append(both(c, side, every, p["b0"], p["b"], sibling))
        if p["d"]:
            for start in (first, second):
                p["pair"].append(both(c, every, every, start, p["d"], sibling))

    def stage4(p):
        c = p["c"]
        for copy in p["s3"]:
            copy.wait_recv()
        if p["a"]:
            p["pair"].append(both(c, every, (y + 2) % 4, p["a0"], p["a"], sibling))
        if p["b"]:
            p["pair"].append(both(c, (zl + 2) % 4, every, p["b0"], p["b"], sibling))
        if p["d"]:
            base = p["d0"] - tp * p["d"]
            start = pl.multiple_of(base + (((x + 2) % 4) * 2 + core) * p["d"], 16)
            p["pair"].append(both(c, every, every, start, p["d"], sibling))

    def stage5(p):
        for copy in p["pair"]:
            copy.wait_recv()

    def norm(s):
        got_tok[s].wait()

        def block(i, carry):
            for half in range(2):
                r = pl.multiple_of(i * 32 + half * 16, 16)
                rows = pl.ds(r, 16)
                tile = lambda j: tok[s, rows, j * 128 : (j + 1) * 128].astype(F32)
                sums = [tile(j) for j in range(4)]
                for j in range(4, 32):
                    sums[j % 4] = sums[j % 4] + tile(j)
                total = (sums[0] + sums[1]) + (sums[2] + sums[3])
                mean = jnp.sum(total, axis=1, keepdims=True) * (1.0 / D)
                squares = [None] * 4
                for j in range(32):
                    gap = tile(j) - mean
                    old = squares[j % 4]
                    squares[j % 4] = gap * gap if old is None else old + gap * gap
                total = (squares[0] + squares[1]) + (squares[2] + squares[3])
                var = jnp.sum(total, axis=1, keepdims=True) * (1.0 / D)
                scale = lax.rsqrt(var + EPS)
                out_rows = pl.ds(pl.multiple_of(s * 128 + r, 16), 16)
                for j in range(32):
                    cols = slice(j * 128, (j + 1) * 128)
                    value = (tile(j) - mean) * scale * gain[:, cols].astype(F32)
                    nrm[out_rows, cols] = value.astype(BF16)
            return carry

        lax.fori_loop(0, 4, block, 0)

    lane = lax.broadcasted_iota(jnp.int32, (64, 128), 1)
    left = lane < HD
    left8 = left[:8]

    def turn(v):
        return pltpu.roll(v, HD, 1)

    def project(c):
        acc[...] = jnp.dot(
            nrm[...], w[c].reshape(D, 256), preferred_element_type=F32
        )
        for s in range(4):
            for p in range(2):
                cols = slice(p * 128, (p + 1) * 128)
                top = acc[s * 128 : s * 128 + 64, cols]
                bottom = acc[s * 128 + 64 : s * 128 + 128, cols]
                even = jnp.where(left, top, turn(bottom))
                odd = jnp.where(left, turn(top), bottom)
                kvs[c, s * 4 + 2 * p] = even.astype(BF16)
                kvs[c, s * 4 + 2 * p + 1] = odd.astype(BF16)
        kvr[c, sp] = kvs[c, sp]
        out = []
        for k in range(1, 16):
            far = at_sp(k)
            out.append(send(kvs.at[c, far[1]], kvr.at[c, sp], far))
        return out

    for p in plan:
        for copy in p["own"]:
            copy.wait()
    stage1(plan[0])
    stage1(plan[1])
    got_gain.wait()
    norm(0)
    stage2(plan[0])
    norm(1)
    stage2(plan[1])
    norm(2)
    stage3(plan[0])
    norm(3)
    stage4(plan[0])
    stage3(plan[1])
    stage5(plan[0])
    moved_k = project(0)
    stage4(plan[1])
    stage5(plan[1])
    moved_v = project(1)

    for copy in got_small:
        copy.wait()
    row8 = lax.broadcasted_iota(jnp.int32, (8, 128), 0)
    qq = jnp.zeros((8, 128), F32)
    for g in range(GROUP):
        part = qv[:, (g // 2) * 128 : (g // 2 + 1) * 128].astype(F32)
        part = jnp.broadcast_to(part, (8, 128))
        other = turn(part)
        mine = jnp.where(left8, part, other) if g % 2 == 0 else jnp.where(left8, other, part)
        qq = jnp.where(row8 == g, mine, qq)
    q_lo = jnp.where(left8, qq, 0.0)
    q_hi = jnp.where(left8, 0.0, qq)
    stack = jnp.concatenate([q_lo, q_hi], axis=0).astype(BF16)
    hrow = lax.broadcasted_iota(jnp.int32, (4, 8), 0)
    own = jnp.sum(jnp.where(hrow == y, hsv[...], 0.0), axis=0, keepdims=True)
    eye = lax.broadcasted_iota(jnp.int32, (8, 8), 0) == lax.broadcasted_iota(jnp.int32, (8, 8), 1)
    head = jnp.sum(jnp.where(eye, jnp.broadcast_to(own, (8, 8)), 0.0), axis=1, keepdims=True)

    for copy in moved_k:
        copy.wait_recv()
    logits = lax.dot_general(
        stack, kvr[0].reshape(1024, 128), (((1,), (1,)), ((), ())), preferred_element_type=F32
    )
    tiles = []
    for m in range(8):
        cols = slice(m * 128, (m + 1) * 128)
        lo, hi = logits[:8, cols], logits[8:, cols]
        tiles.append(jnp.where(left8, lo, turn(hi)))
        tiles.append(jnp.where(left8, turn(lo), hi))
    z_all = jnp.concatenate(
        [
            t * HD ** (-0.5) + head + ksv[:, n * 128 : (n + 1) * 128]
            for n, t in enumerate(tiles)
        ],
        axis=0,
    )
    log_beta = jnp.minimum(z_all, 0.0) - jnp.log1p(jnp.exp(-jnp.abs(z_all)))
    log_keep = log_beta - z_all
    ri = lax.broadcasted_iota(jnp.int32, (128, 256), 0)
    ci = lax.broadcasted_iota(jnp.int32, (128, 256), 1)
    later = jnp.where((ci >= 128) | (ri > ci), 1.0, 0.0).astype(F32)
    sums = jnp.dot(
        log_keep, later, preferred_element_type=F32, precision=lax.Precision.HIGHEST
    )
    tail = jnp.zeros((8, 128), F32)
    weights = [None] * 16
    for n in reversed(range(16)):
        rows = slice(n * 8, (n + 1) * 8)
        weights[n] = jnp.exp(log_beta[rows] + (sums[rows, :128] + tail))
        tail = tail + sums[rows, 128:]
    w_lo = [jnp.where(left8, weights[2 * m], turn(weights[2 * m + 1])) for m in range(8)]
    w_hi = [jnp.where(left8, turn(weights[2 * m]), weights[2 * m + 1]) for m in range(8)]
    wstack = jnp.concatenate(
        [jnp.concatenate(w_lo, axis=1), jnp.concatenate(w_hi, axis=1)], axis=0
    ).astype(BF16)

    for copy in moved_v:
        copy.wait_recv()
    out = jnp.dot(wstack, kvr[1].reshape(1024, 128), preferred_element_type=F32)
    section = out[:8] + turn(out[8:])
    message = jnp.where(left8, section, tail)
    xs[...] = message
    xr[tp] = message
    shared = [send(xs, xr.at[tp], at_tp(k)) for k in range(1, 8)]

    def assemble(j, carry):
        keys = kvr[0, j].astype(F32)
        values = kvr[1, j].astype(F32)
        first = pl.multiple_of(j * 128, 64)
        second = pl.multiple_of(j * 128 + 64, 64)
        cache[pl.ds(first, 64), :] = jnp.where(left, keys, turn(values)).astype(BF16)
        cache[pl.ds(second, 64), :] = jnp.where(left, turn(keys), values).astype(BF16)
        return carry

    lax.fori_loop(0, 16, assemble, 0)
    stored = fetch(cache, cache_hbm.at[0])

    for copy in shared:
        copy.wait_recv()
    carry = jnp.zeros((8, 128), F32)
    result = jnp.zeros((8, 128), F32)
    for t in reversed(range(8)):
        tile = xr[t]
        result = result + jnp.exp(carry) * tile
        carry = carry + turn(tile)
    result = jnp.where(left8, result, turn(result))
    for k in range(4):
        rdv[:, k * 128 : (k + 1) * 128] = jnp.where(
            left8[:1], result[2 * k : 2 * k + 1], result[2 * k + 1 : 2 * k + 2]
        )
    answered = fetch(rdv, read_hbm)
    for copy in copies:
        copy.wait_send()
    stored.wait()
    answered.wait()


def local(tokens, ln_gain, w_key, w_value, queries, head_shift, key_shift):
    any_ = pl.BlockSpec(memory_space=pl.ANY)
    return pl.pallas_call(
        kernel,
        out_shape=(
            jax.ShapeDtypeStruct((1, 2048, 128), BF16),
            jax.ShapeDtypeStruct((1, 512), F32),
        ),
        in_specs=[any_] * 7,
        out_specs=(any_, any_),
        scratch_shapes=[
            pltpu.VMEM((4, 128, D), BF16),
            pltpu.VMEM((512, D), BF16),
            pltpu.VMEM((2, 4, 4, 256, 256), BF16),
            pltpu.VMEM((512, 256), F32),
            pltpu.VMEM((2, 16, 64, 128), BF16),
            pltpu.VMEM((2, 16, 64, 128), BF16),
            pltpu.VMEM((2048, 128), BF16),
            pltpu.VMEM((1, D), BF16),
            pltpu.VMEM((1, 512), BF16),
            pltpu.VMEM((4, 8), F32),
            pltpu.VMEM((1, 2048), F32),
            pltpu.VMEM((1, 512), F32),
            pltpu.VMEM((8, 128), F32),
            pltpu.VMEM((8, 8, 128), F32),
            pltpu.SemaphoreType.DMA((16,)),
            pltpu.SemaphoreType.DMA((MAX_COPIES,)),
            pltpu.SemaphoreType.DMA((MAX_COPIES,)),
        ],
        compiler_params=pltpu.CompilerParams(collective_id=0, has_side_effects=True),
    )(tokens, ln_gain.reshape(1, D), w_key, w_value, queries, head_shift, key_shift)


def solution(mesh):
    placed = (
        P("gr", "tp", "sp", None),
        P(),
        P("sp", None),
        P("sp", None),
        P(("gr", "sp"), None),
        P(),
        P(("gr", "sp"), "tp"),
    )
    return jax.shard_map(
        local,
        mesh=mesh,
        in_specs=placed,
        out_specs=(P(("gr", "sp"), "tp", None), P(("gr", "sp"), None)),
        check_vma=False,
    )
```

```python
import functools

import jax
import jax.numpy as jnp
from jax import lax
from jax.experimental import pallas as pl
from jax.experimental.pallas import tpu as pltpu
from jax.sharding import PartitionSpec as P

MESH = pl.DeviceIdType.MESH
F32, BF16 = jnp.float32, jnp.bfloat16
D, HD, KVH, GROUP = 4096, 64, 4, 8
EPS = 1e-05
SPLIT = (128, 128)
MAX_COPIES = 128


class Line:
    def __init__(self, c, way, rows):
        self.c, self.way, self.rows = c, way, rows


def kernel(
    tok_hbm, gain_hbm, wk_hbm, wv_hbm, q_hbm, hs_hbm, ks_hbm,
    cache_hbm, read_hbm,
    tok, nrm, w, acc, kvs, kvr, cache, gain, qv, hsv, ksv, rdv, xs, xr,
    local_sem, send_sem, recv_sem,
):
    gr, sp, tp = lax.axis_index("gr"), lax.axis_index("sp"), lax.axis_index("tp")
    x, core = tp // 2, tp % 2
    zl, y = sp // 4, sp % 4
    z = gr * 4 + zl

    def at_z(k):
        far = (z + k) % 8
        return (far // 4, (far % 4) * 4 + y, tp)

    def at_y(k):
        return (gr, zl * 4 + (y + k) % 4, tp)

    def at_sp(k):
        return (gr, (sp + k) % 16, tp)

    def at_tp(k):
        return (gr, sp, (tp + k) % 8)

    sibling = (gr, sp, x * 2 + 1 - core)

    copies = []

    def send(src, dst, device):
        number = len(copies)
        copy = pltpu.make_async_remote_copy(
            src_ref=src,
            dst_ref=dst,
            send_sem=send_sem.at[number],
            recv_sem=recv_sem.at[number],
            device_id=device,
            device_id_type=MESH,
        )
        copy.start()
        copies.append(copy)
        return copy

    locals_ = []

    def fetch(src, dst):
        copy = pltpu.make_async_copy(src, dst, local_sem.at[len(locals_)])
        copy.start()
        locals_.append(copy)
        return copy

    lines = []
    for c in range(2):
        first = SPLIT[c]
        for way, (start, count) in enumerate(((0, first), (first, 256 - first))):
            if count == 0:
                continue
            rows = pl.ds(pl.multiple_of(start + core * (count // 2), 16), count // 2)
            lines.append(Line(c, way, rows))
    for line in lines:
        source = (wk_hbm, wv_hbm)[line.c].at[line.rows, :]
        line.own = fetch(source, w.at[line.c, zl, y, line.rows, :])
    got_gain = fetch(gain_hbm, gain)
    got_tok = [fetch(tok_hbm.at[s, 0], tok.at[s]) for s in range(4)]
    got_small = [fetch(q_hbm, qv), fetch(hs_hbm, hsv), fetch(ks_hbm, ksv)]

    barrier = pltpu.get_barrier_semaphore()
    friends = [at_z(k) for k in (1, -1, 2, -2)]
    friends += [at_y(k) for k in (1, -1, 2)]
    friends += [at_tp(k) for k in range(1, 8)]
    for friend in friends:
        pl.semaphore_signal(barrier, inc=1, device_id=friend, device_id_type=MESH)
    pl.semaphore_wait(barrier, len(friends))

    every = pl.ds(0, 4)
    side = 1 - 2 * core

    def shift(line, i, j):
        mine = (zl, y) if line.way == 0 else (y, zl)
        return tuple(
            v if k is None else v if isinstance(k, int) and k == 0 else (v + k + 4) % 4
            for v, k in zip(mine, (i, j))
        )

    def pass_on(line, i, j, device):
        a, b = (every if k is None else v for k, v in zip((i, j), shift(line, i, j)))
        if line.way == 1:
            a, b = b, a
        ref = w.at[line.c, a, b, line.rows, :]
        return send(ref, ref, device)

    def one(line, k):
        return at_z(k) if line.way == 0 else at_y(k)

    def two(line, k):
        return at_y(k) if line.way == 0 else at_z(k)

    def wave0(line):
        line.own.wait()
        far = 2 * side if line.way == 0 else 2
        line.far = pass_on(line, 0, 0, one(line, far))
        line.near = [pass_on(line, 0, 0, one(line, k)) for k in (1, -1)]
        line.side = {0: [pass_on(line, 0, 0, two(line, k)) for k in (1, -1)]}

    def wave1(line):
        for copy, i in zip(line.near, (-1, 1)):
            copy.wait_recv()
            line.side[i] = [pass_on(line, i, 0, two(line, k)) for k in (1, -1)]

    def wave2(line):
        line.far.wait_recv()
        line.side[2] = [pass_on(line, 2, 0, two(line, k)) for k in (1, -1)]
        line.pair = [pass_on(line, None, 0, sibling)]

    def wave3(line):
        line.relay = []
        for i in (0, -1, 1):
            for copy in line.side[i]:
                copy.wait_recv()
            way = side if i == 0 else -side
            line.relay.append(pass_on(line, i, -way, two(line, way)))

    def wave4(line):
        for copy in line.side[2]:
            copy.wait_recv()
        line.relay.append(pass_on(line, 2, -side, two(line, side)))
        line.pair += [pass_on(line, None, k, sibling) for k in (-1, 1)]

    def wave5(line):
        for copy in line.relay:
            copy.wait_recv()
        line.pair.append(pass_on(line, None, 2, sibling))

    def wave6(line):
        for copy in line.pair:
            copy.wait_recv()

    def norm(s):
        got_tok[s].wait()

        def block(i, carry):
            for half in range(2):
                r = pl.multiple_of(i * 32 + half * 16, 16)
                rows = pl.ds(r, 16)
                tile = lambda j: tok[s, rows, j * 128 : (j + 1) * 128].astype(F32)
                sums = [tile(j) for j in range(4)]
                for j in range(4, 32):
                    sums[j % 4] = sums[j % 4] + tile(j)
                total = (sums[0] + sums[1]) + (sums[2] + sums[3])
                mean = jnp.sum(total, axis=1, keepdims=True) * (1.0 / D)
                squares = [None] * 4
                for j in range(32):
                    gap = tile(j) - mean
                    old = squares[j % 4]
                    squares[j % 4] = gap * gap if old is None else old + gap * gap
                total = (squares[0] + squares[1]) + (squares[2] + squares[3])
                var = jnp.sum(total, axis=1, keepdims=True) * (1.0 / D)
                scale = lax.rsqrt(var + EPS)
                out_rows = pl.ds(pl.multiple_of(s * 128 + r, 16), 16)
                for j in range(32):
                    cols = slice(j * 128, (j + 1) * 128)
                    value = (tile(j) - mean) * scale * gain[cols].astype(F32).reshape(1, 128)
                    nrm[out_rows, cols] = value.astype(BF16)
            return carry

        lax.fori_loop(0, 4, block, 0)

    lane = lax.broadcasted_iota(jnp.int32, (64, 128), 1)
    left = lane < HD
    left8 = left[:8]

    def turn(v):
        return pltpu.roll(v, HD, 1)

    def project(c):
        acc[...] = jnp.dot(
            nrm[...], w[c].reshape(D, 256), preferred_element_type=F32
        )
        for s in range(4):
            for p in range(2):
                cols = slice(p * 128, (p + 1) * 128)
                top = acc[s * 128 : s * 128 + 64, cols]
                bottom = acc[s * 128 + 64 : s * 128 + 128, cols]
                even = jnp.where(left, top, turn(bottom))
                odd = jnp.where(left, turn(top), bottom)
                kvs[c, s * 4 + 2 * p] = even.astype(BF16)
                kvs[c, s * 4 + 2 * p + 1] = odd.astype(BF16)
        kvr[c, sp] = kvs[c, sp]
        out = []
        for k in range(1, 16):
            far = at_sp(k)
            out.append(send(kvs.at[c, far[1]], kvr.at[c, sp], far))
        return out

    k_lines = [line for line in lines if line.c == 0]
    v_lines = [line for line in lines if line.c == 1]

    def each(wave, some):
        for line in some:
            wave(line)

    each(wave0, k_lines)
    each(wave0, v_lines)
    got_gain.wait()
    norm(0)
    each(wave1, k_lines)
    norm(1)
    each(wave2, k_lines)
    each(wave1, v_lines)
    norm(2)
    each(wave3, k_lines)
    each(wave2, v_lines)
    norm(3)
    each(wave4, k_lines)
    each(wave3, v_lines)
    each(wave5, k_lines)
    each(wave4, v_lines)
    each(wave6, k_lines)
    moved_k = project(0)
    each(wave5, v_lines)
    each(wave6, v_lines)
    moved_v = project(1)

    for copy in got_small:
        copy.wait()
    row8 = lax.broadcasted_iota(jnp.int32, (8, 128), 0)
    qq = jnp.zeros((8, 128), F32)
    for g in range(GROUP):
        part = qv[:, (g // 2) * 128 : (g // 2 + 1) * 128].astype(F32)
        part = jnp.broadcast_to(part, (8, 128))
        other = turn(part)
        mine = jnp.where(left8, part, other) if g % 2 == 0 else jnp.where(left8, other, part)
        qq = jnp.where(row8 == g, mine, qq)
    q_lo = jnp.where(left8, qq, 0.0)
    q_hi = jnp.where(left8, 0.0, qq)
    stack = jnp.concatenate([q_lo, q_hi], axis=0).astype(BF16)
    hrow = lax.broadcasted_iota(jnp.int32, (4, 8), 0)
    own = jnp.sum(jnp.where(hrow == y, hsv[...], 0.0), axis=0, keepdims=True)
    eye = lax.broadcasted_iota(jnp.int32, (8, 8), 0) == lax.broadcasted_iota(jnp.int32, (8, 8), 1)
    head = jnp.sum(jnp.where(eye, jnp.broadcast_to(own, (8, 8)), 0.0), axis=1, keepdims=True)

    for copy in moved_k:
        copy.wait_recv()
    logits = lax.dot_general(
        stack, kvr[0].reshape(1024, 128), (((1,), (1,)), ((), ())), preferred_element_type=F32
    )
    tiles = []
    for m in range(8):
        cols = slice(m * 128, (m + 1) * 128)
        lo, hi = logits[:8, cols], logits[8:, cols]
        tiles.append(jnp.where(left8, lo, turn(hi)))
        tiles.append(jnp.where(left8, turn(lo), hi))
    z_all = jnp.concatenate(
        [
            t * HD ** (-0.5) + head + ksv[:, n * 128 : (n + 1) * 128]
            for n, t in enumerate(tiles)
        ],
        axis=0,
    )
    log_beta = jnp.minimum(z_all, 0.0) - jnp.log1p(jnp.exp(-jnp.abs(z_all)))
    log_keep = log_beta - z_all
    ri = lax.broadcasted_iota(jnp.int32, (128, 256), 0)
    ci = lax.broadcasted_iota(jnp.int32, (128, 256), 1)
    later = jnp.where((ci >= 128) | (ri > ci), 1.0, 0.0).astype(F32)
    sums = jnp.dot(
        log_keep, later, preferred_element_type=F32, precision=lax.Precision.HIGHEST
    )
    tail = jnp.zeros((8, 128), F32)
    weights = [None] * 16
    for n in reversed(range(16)):
        rows = slice(n * 8, (n + 1) * 8)
        weights[n] = jnp.exp(log_beta[rows] + (sums[rows, :128] + tail))
        tail = tail + sums[rows, 128:]
    w_lo = [jnp.where(left8, weights[2 * m], turn(weights[2 * m + 1])) for m in range(8)]
    w_hi = [jnp.where(left8, turn(weights[2 * m]), weights[2 * m + 1]) for m in range(8)]
    wstack = jnp.concatenate(
        [jnp.concatenate(w_lo, axis=1), jnp.concatenate(w_hi, axis=1)], axis=0
    ).astype(BF16)

    for copy in moved_v:
        copy.wait_recv()
    out = jnp.dot(wstack, kvr[1].reshape(1024, 128), preferred_element_type=F32)
    section = out[:8] + turn(out[8:])
    message = jnp.where(left8, section, tail)
    xs[...] = message
    xr[tp] = message
    shared = [send(xs, xr.at[tp], at_tp(k)) for k in range(1, 8)]

    def assemble(j, carry):
        keys = kvr[0, j].astype(F32)
        values = kvr[1, j].astype(F32)
        first = pl.multiple_of(j * 128, 64)
        second = pl.multiple_of(j * 128 + 64, 64)
        cache[pl.ds(first, 64), :] = jnp.where(left, keys, turn(values)).astype(BF16)
        cache[pl.ds(second, 64), :] = jnp.where(left, turn(keys), values).astype(BF16)
        return carry

    lax.fori_loop(0, 16, assemble, 0)
    stored = fetch(cache, cache_hbm.at[0])

    for copy in shared:
        copy.wait_recv()
    carry = jnp.zeros((8, 128), F32)
    result = jnp.zeros((8, 128), F32)
    for t in reversed(range(8)):
        tile = xr[t]
        result = result + jnp.exp(carry) * tile
        carry = carry + turn(tile)
    result = jnp.where(left8, result, turn(result))
    for k in range(4):
        rdv[:, k * 128 : (k + 1) * 128] = jnp.where(
            left8[:1], result[2 * k : 2 * k + 1], result[2 * k + 1 : 2 * k + 2]
        )
    answered = fetch(rdv, read_hbm)
    for copy in copies:
        copy.wait_send()
    stored.wait()
    answered.wait()


def local(tokens, ln_gain, w_key, w_value, queries, head_shift, key_shift):
    any_ = pl.BlockSpec(memory_space=pl.ANY)
    return pl.pallas_call(
        kernel,
        out_shape=(
            jax.ShapeDtypeStruct((1, 2048, 128), BF16),
            jax.ShapeDtypeStruct((1, 512), F32),
        ),
        in_specs=[any_] * 7,
        out_specs=(any_, any_),
        scratch_shapes=[
            pltpu.VMEM((4, 128, D), BF16),
            pltpu.VMEM((512, D), BF16),
            pltpu.VMEM((2, 4, 4, 256, 256), BF16),
            pltpu.VMEM((512, 256), F32),
            pltpu.VMEM((2, 16, 64, 128), BF16),
            pltpu.VMEM((2, 16, 64, 128), BF16),
            pltpu.VMEM((2048, 128), BF16),
            pltpu.VMEM((D,), BF16),
            pltpu.VMEM((1, 512), BF16),
            pltpu.VMEM((4, 8), F32),
            pltpu.VMEM((1, 2048), F32),
            pltpu.VMEM((1, 512), F32),
            pltpu.VMEM((8, 128), F32),
            pltpu.VMEM((8, 8, 128), F32),
            pltpu.SemaphoreType.DMA((16,)),
            pltpu.SemaphoreType.DMA((MAX_COPIES,)),
            pltpu.SemaphoreType.DMA((MAX_COPIES,)),
        ],
        compiler_params=pltpu.CompilerParams(collective_id=0, has_side_effects=True),
    )(tokens, ln_gain, w_key, w_value, queries, head_shift, key_shift)


def solution(mesh):
    placed = (
        P("gr", "tp", "sp", None),
        P(),
        P("sp", None),
        P("sp", None),
        P(("gr", "sp"), None),
        P(),
        P(("gr", "sp"), "tp"),
    )
    return jax.shard_map(
        local,
        mesh=mesh,
        in_specs=placed,
        out_specs=(P(("gr", "sp"), "tp", None), P(("gr", "sp"), None)),
        check_vma=False,
    )
```

```python
import functools

import jax
import jax.numpy as jnp
from jax import lax
from jax.experimental import pallas as pl
from jax.experimental.pallas import tpu as pltpu
from jax.sharding import PartitionSpec as P

MESH = pl.DeviceIdType.MESH
F32, BF16 = jnp.float32, jnp.bfloat16
D, HD, KVH, GROUP = 4096, 64, 4, 8
EPS = 1e-05
SPLIT = (128, 128)
LINES, PER_LINE = 4, 7
NEAR, FAR, SECOND, PAIR, SENT = 0, 1, (2, 3, 4), 5, 6
BLOCKS, BLOCKS_SENT = LINES * PER_LINE, LINES * PER_LINE + 2
SHARED, SHARED_SENT = BLOCKS + 4, BLOCKS + 5
SEMAPHORES = BLOCKS + 6


class Line:
    def __init__(self, number, c, way, rows):
        self.number, self.c, self.way, self.rows = number, c, way, rows


def kernel(
    tok_hbm, gain_hbm, wk_hbm, wv_hbm, q_hbm, hs_hbm, ks_hbm,
    cache_hbm, read_hbm,
    tok, nrm, w, acc, kvs, kvr, cache, gain, qv, hsv, ksv, rdv, xs, xr,
    ruler, local_sem, sems,
):
    gr, sp, tp = lax.axis_index("gr"), lax.axis_index("sp"), lax.axis_index("tp")
    x, core = tp // 2, tp % 2
    zl, y = sp // 4, sp % 4
    z = gr * 4 + zl

    def at_z(k):
        far = (z + k) % 8
        return (far // 4, (far % 4) * 4 + y, tp)

    def at_y(k):
        return (gr, zl * 4 + (y + k) % 4, tp)

    def at_sp(k):
        return (gr, (sp + k) % 16, tp)

    def at_tp(k):
        return (gr, sp, (tp + k) % 8)

    sibling = (gr, sp, x * 2 + 1 - core)

    def send(src, dst, device, sent, arrived):
        pltpu.make_async_remote_copy(
            src_ref=src,
            dst_ref=dst,
            send_sem=sems.at[sent],
            recv_sem=sems.at[arrived],
            device_id=device,
            device_id_type=MESH,
        ).start()

    def take(number, kib):
        span = ruler.at[pl.ds(0, kib * 4), :]
        pltpu.make_async_copy(span, span, sems.at[number]).wait()

    locals_ = []

    def fetch(src, dst):
        copy = pltpu.make_async_copy(src, dst, local_sem.at[len(locals_)])
        copy.start()
        locals_.append(copy)
        return copy

    lines = []
    for c in range(2):
        for way in range(2):
            start = pl.multiple_of(way * SPLIT[0] + core * (SPLIT[way] // 2), 32)
            lines.append(Line(len(lines), c, way, pl.ds(start, SPLIT[way] // 2)))
            lines[-1].kib = SPLIT[way] // 4
    for line in lines:
        source = (wk_hbm, wv_hbm)[line.c].at[line.rows, :]
        line.own = fetch(source, w.at[line.c, zl, y, line.rows, :])
    got_gain = fetch(gain_hbm, gain)
    got_tok = [fetch(tok_hbm.at[s, 0], tok.at[s]) for s in range(4)]
    got_small = [fetch(q_hbm, qv), fetch(hs_hbm, hsv), fetch(ks_hbm, ksv)]

    barrier = pltpu.get_barrier_semaphore()
    friends = [at_z(k) for k in (1, -1, 2, -2)]
    friends += [at_y(k) for k in (1, -1, 2)]
    friends += [at_tp(k) for k in range(1, 8)]
    for friend in friends:
        pl.semaphore_signal(barrier, inc=1, device_id=friend, device_id_type=MESH)
    pl.semaphore_wait(barrier, len(friends))

    every = pl.ds(0, 4)
    side = 1 - 2 * core

    def shift(line, i, j):
        mine = (y, zl) if line.way == 1 else (zl, y)
        return tuple(
            v if k is None else v if isinstance(k, int) and k == 0 else (v + k + 4) % 4
            for v, k in zip(mine, (i, j))
        )

    def pass_on(line, i, j, device, kind):
        a, b = (every if k is None else v for k, v in zip((i, j), shift(line, i, j)))
        if line.way == 1:
            a, b = b, a
        ref = w.at[line.c, a, b, line.rows, :]
        base = line.number * PER_LINE
        send(ref, ref, device, base + SENT, base + kind)

    def arrived(line, kind, pieces):
        take(line.number * PER_LINE + kind, pieces * line.kib)

    def one(line, k):
        return at_y(k) if line.way == 1 else at_z(k)

    def two(line, k):
        return at_z(k) if line.way == 1 else at_y(k)

    def offsets(along_z):
        return (2 * side if along_z else 2, 1, -1)

    def along(line, i):
        for k, kind in zip(offsets(line.way == 1), SECOND):
            pass_on(line, i, 0, two(line, k), kind)

    def wave0(line):
        line.own.wait()
        for k, kind in zip(offsets(line.way == 0), (FAR, NEAR, NEAR)):
            pass_on(line, 0, 0, one(line, k), kind)

    def wave1(line):
        along(line, 0)

    def wave2(line):
        arrived(line, NEAR, 2)
        along(line, -1)
        along(line, 1)

    def wave3(line):
        arrived(line, FAR, 1)
        along(line, 2)
        pass_on(line, None, 0, sibling, PAIR)

    def wave4(line):
        for n, j in ((1, -1), (2, 1), (0, 2)):
            arrived(line, SECOND[n], 4)
            pass_on(line, None, j, sibling, PAIR)

    def wave5(line):
        arrived(line, PAIR, 16)

    def norm(s):
        got_tok[s].wait()

        def block(i, carry):
            for half in range(2):
                r = pl.multiple_of(i * 32 + half * 16, 16)
                rows = pl.ds(r, 16)
                tile = lambda j: tok[s, rows, j * 128 : (j + 1) * 128].astype(F32)
                sums = [tile(j) for j in range(4)]
                for j in range(4, 32):
                    sums[j % 4] = sums[j % 4] + tile(j)
                total = (sums[0] + sums[1]) + (sums[2] + sums[3])
                mean = jnp.sum(total, axis=1, keepdims=True) * (1.0 / D)
                squares = [None] * 4
                for j in range(32):
                    gap = tile(j) - mean
                    old = squares[j % 4]
                    squares[j % 4] = gap * gap if old is None else old + gap * gap
                total = (squares[0] + squares[1]) + (squares[2] + squares[3])
                var = jnp.sum(total, axis=1, keepdims=True) * (1.0 / D)
                scale = lax.rsqrt(var + EPS)
                out_rows = pl.ds(pl.multiple_of(s * 128 + r, 16), 16)
                for j in range(32):
                    cols = slice(j * 128, (j + 1) * 128)
                    value = (tile(j) - mean) * scale * gain[cols].astype(F32).reshape(1, 128)
                    nrm[out_rows, cols] = value.astype(BF16)
            return carry

        lax.fori_loop(0, 4, block, 0)

    lane = lax.broadcasted_iota(jnp.int32, (64, 128), 1)
    left = lane < HD
    left8 = left[:8]

    def turn(v):
        return pltpu.roll(v, HD, 1)

    def project(c):
        acc[...] = jnp.dot(
            nrm[...], w[c].reshape(D, 256), preferred_element_type=F32
        )
        for s in range(4):
            for p in range(2):
                cols = slice(p * 128, (p + 1) * 128)
                top = acc[s * 128 : s * 128 + 64, cols]
                bottom = acc[s * 128 + 64 : s * 128 + 128, cols]
                even = jnp.where(left, top, turn(bottom))
                odd = jnp.where(left, turn(top), bottom)
                kvs[c, s * 4 + 2 * p] = even.astype(BF16)
                kvs[c, s * 4 + 2 * p + 1] = odd.astype(BF16)
        kvr[c, sp] = kvs[c, sp]
        for k in range(1, 16):
            far = at_sp(k)
            send(kvs.at[c, far[1]], kvr.at[c, sp], far, BLOCKS_SENT + c, BLOCKS + c)

    k_lines = [line for line in lines if line.c == 0]
    v_lines = [line for line in lines if line.c == 1]

    def each(wave, some):
        for line in some:
            wave(line)

    each(wave0, k_lines)
    got_gain.wait()
    norm(0)
    each(wave1, k_lines)
    each(wave2, k_lines)
    each(wave3, k_lines)
    each(wave0, v_lines)
    norm(1)
    each(wave1, v_lines)
    norm(2)
    each(wave2, v_lines)
    norm(3)
    each(wave3, v_lines)
    each(wave4, k_lines)
    each(wave5, k_lines)
    project(0)
    each(wave4, v_lines)
    each(wave5, v_lines)
    project(1)

    for copy in got_small:
        copy.wait()
    row8 = lax.broadcasted_iota(jnp.int32, (8, 128), 0)
    qq = jnp.zeros((8, 128), F32)
    for g in range(GROUP):
        part = qv[:, (g // 2) * 128 : (g // 2 + 1) * 128].astype(F32)
        part = jnp.broadcast_to(part, (8, 128))
        other = turn(part)
        mine = jnp.where(left8, part, other) if g % 2 == 0 else jnp.where(left8, other, part)
        qq = jnp.where(row8 == g, mine, qq)
    q_lo = jnp.where(left8, qq, 0.0)
    q_hi = jnp.where(left8, 0.0, qq)
    stack = jnp.concatenate([q_lo, q_hi], axis=0).astype(BF16)
    hrow = lax.broadcasted_iota(jnp.int32, (4, 8), 0)
    own = jnp.sum(jnp.where(hrow == y, hsv[...], 0.0), axis=0, keepdims=True)
    eye = lax.broadcasted_iota(jnp.int32, (8, 8), 0) == lax.broadcasted_iota(jnp.int32, (8, 8), 1)
    head = jnp.sum(jnp.where(eye, jnp.broadcast_to(own, (8, 8)), 0.0), axis=1, keepdims=True)

    take(BLOCKS, 240)
    logits = lax.dot_general(
        stack, kvr[0].reshape(1024, 128), (((1,), (1,)), ((), ())), preferred_element_type=F32
    )
    tiles = []
    for m in range(8):
        cols = slice(m * 128, (m + 1) * 128)
        lo, hi = logits[:8, cols], logits[8:, cols]
        tiles.append(jnp.where(left8, lo, turn(hi)))
        tiles.append(jnp.where(left8, turn(lo), hi))
    z_all = jnp.concatenate(
        [
            t * HD ** (-0.5) + head + ksv[:, n * 128 : (n + 1) * 128]
            for n, t in enumerate(tiles)
        ],
        axis=0,
    )
    log_beta = jnp.minimum(z_all, 0.0) - jnp.log1p(jnp.exp(-jnp.abs(z_all)))
    log_keep = log_beta - z_all
    ri = lax.broadcasted_iota(jnp.int32, (128, 256), 0)
    ci = lax.broadcasted_iota(jnp.int32, (128, 256), 1)
    later = jnp.where((ci >= 128) | (ri > ci), 1.0, 0.0).astype(F32)
    sums = jnp.dot(
        log_keep, later, preferred_element_type=F32, precision=lax.Precision.HIGHEST
    )
    tail = jnp.zeros((8, 128), F32)
    weights = [None] * 16
    for n in reversed(range(16)):
        rows = slice(n * 8, (n + 1) * 8)
        weights[n] = jnp.exp(log_beta[rows] + (sums[rows, :128] + tail))
        tail = tail + sums[rows, 128:]
    w_lo = [jnp.where(left8, weights[2 * m], turn(weights[2 * m + 1])) for m in range(8)]
    w_hi = [jnp.where(left8, turn(weights[2 * m]), weights[2 * m + 1]) for m in range(8)]
    wstack = jnp.concatenate(
        [jnp.concatenate(w_lo, axis=1), jnp.concatenate(w_hi, axis=1)], axis=0
    ).astype(BF16)

    take(BLOCKS + 1, 240)
    out = jnp.dot(wstack, kvr[1].reshape(1024, 128), preferred_element_type=F32)
    section = out[:8] + turn(out[8:])
    message = jnp.where(left8, section, tail)
    xs[...] = message
    xr[tp] = message
    for k in range(1, 8):
        send(xs, xr.at[tp], at_tp(k), SHARED_SENT, SHARED)

    def assemble(j, carry):
        keys = kvr[0, j].astype(F32)
        values = kvr[1, j].astype(F32)
        first = pl.multiple_of(j * 128, 64)
        second = pl.multiple_of(j * 128 + 64, 64)
        cache[pl.ds(first, 64), :] = jnp.where(left, keys, turn(values)).astype(BF16)
        cache[pl.ds(second, 64), :] = jnp.where(left, turn(keys), values).astype(BF16)
        return carry

    lax.fori_loop(0, 16, assemble, 0)
    stored = fetch(cache, cache_hbm.at[0])

    take(SHARED, 28)
    carry = jnp.zeros((8, 128), F32)
    result = jnp.zeros((8, 128), F32)
    for t in reversed(range(8)):
        tile = xr[t]
        result = result + jnp.exp(carry) * tile
        carry = carry + turn(tile)
    result = jnp.where(left8, result, turn(result))
    for k in range(4):
        rdv[:, k * 128 : (k + 1) * 128] = jnp.where(
            left8[:1], result[2 * k : 2 * k + 1], result[2 * k + 1 : 2 * k + 2]
        )
    answered = fetch(rdv, read_hbm)
    for line in lines:
        take(line.number * PER_LINE + SENT, 31 * line.kib)
    for c in range(2):
        take(BLOCKS_SENT + c, 240)
    take(SHARED_SENT, 28)
    stored.wait()
    answered.wait()


def local(tokens, ln_gain, w_key, w_value, queries, head_shift, key_shift):
    any_ = pl.BlockSpec(memory_space=pl.ANY)
    return pl.pallas_call(
        kernel,
        out_shape=(
            jax.ShapeDtypeStruct((1, 2048, 128), BF16),
            jax.ShapeDtypeStruct((1, 512), F32),
        ),
        in_specs=[any_] * 7,
        out_specs=(any_, any_),
        scratch_shapes=[
            pltpu.VMEM((4, 128, D), BF16),
            pltpu.VMEM((512, D), BF16),
            pltpu.VMEM((2, 4, 4, 256, 256), BF16),
            pltpu.VMEM((512, 256), F32),
            pltpu.VMEM((2, 16, 64, 128), BF16),
            pltpu.VMEM((2, 16, 64, 128), BF16),
            pltpu.VMEM((2048, 128), BF16),
            pltpu.VMEM((D,), BF16),
            pltpu.VMEM((1, 512), BF16),
            pltpu.VMEM((4, 8), F32),
            pltpu.VMEM((1, 2048), F32),
            pltpu.VMEM((1, 512), F32),
            pltpu.VMEM((8, 128), F32),
            pltpu.VMEM((8, 8, 128), F32),
            pltpu.VMEM((4096, 128), BF16),
            pltpu.SemaphoreType.DMA((14,)),
            pltpu.SemaphoreType.DMA((SEMAPHORES,)),
        ],
        compiler_params=pltpu.CompilerParams(collective_id=0, has_side_effects=True),
    )(tokens, ln_gain, w_key, w_value, queries, head_shift, key_shift)


def solution(mesh):
    placed = (
        P("gr", "tp", "sp", None),
        P(),
        P("sp", None),
        P("sp", None),
        P(("gr", "sp"), None),
        P(),
        P(("gr", "sp"), "tp"),
    )
    return jax.shard_map(
        local,
        mesh=mesh,
        in_specs=placed,
        out_specs=(P(("gr", "sp"), "tp", None), P(("gr", "sp"), None)),
        check_vma=False,
    )
```

```python
import functools

import jax
import jax.numpy as jnp
from jax import lax
from jax.experimental import pallas as pl
from jax.experimental.pallas import tpu as pltpu
from jax.sharding import PartitionSpec as P

MESH = pl.DeviceIdType.MESH
F32, BF16 = jnp.float32, jnp.bfloat16
D, HD, KVH, GROUP = 4096, 64, 4, 8
EPS = 1e-05
SPLIT = (128, 128)
LINES, PER_LINE = 4, 7
NEAR, FAR, SECOND, PAIR, SENT = 0, 1, (2, 3, 4), 5, 6
BLOCKS, BLOCKS_SENT = LINES * PER_LINE, LINES * PER_LINE + 2
SHARED, SHARED_SENT = BLOCKS + 4, BLOCKS + 5
SEMAPHORES = BLOCKS + 6


class Line:
    def __init__(self, number, c, way, rows):
        self.number, self.c, self.way, self.rows = number, c, way, rows


def kernel(
    tok_hbm, gain_hbm, wk_hbm, wv_hbm, q_hbm, hs_hbm, ks_hbm,
    cache_hbm, read_hbm,
    tok, nrm, w, acc, kvs, kvr, cache, gain, qv, hsv, ksv, rdv, xs, xr,
    ruler, local_sem, sems,
):
    gr, sp, tp = lax.axis_index("gr"), lax.axis_index("sp"), lax.axis_index("tp")
    x, core = tp // 2, tp % 2
    zl, y = sp // 4, sp % 4
    z = gr * 4 + zl

    def at_z(k):
        far = (z + k) % 8
        return (far // 4, (far % 4) * 4 + y, tp)

    def at_y(k):
        return (gr, zl * 4 + (y + k) % 4, tp)

    def at_sp(k):
        return (gr, (sp + k) % 16, tp)

    def at_tp(k):
        return (gr, sp, (tp + k) % 8)

    sibling = (gr, sp, x * 2 + 1 - core)

    def send(src, dst, device, sent, arrived):
        pltpu.make_async_remote_copy(
            src_ref=src,
            dst_ref=dst,
            send_sem=sems.at[sent],
            recv_sem=sems.at[arrived],
            device_id=device,
            device_id_type=MESH,
        ).start()

    def take(number, kib):
        span = ruler.at[pl.ds(0, kib * 4), :]
        pltpu.make_async_copy(span, span, sems.at[number]).wait()

    locals_ = []

    def fetch(src, dst):
        copy = pltpu.make_async_copy(src, dst, local_sem.at[len(locals_)])
        copy.start()
        locals_.append(copy)
        return copy

    lines = []
    for c in range(2):
        for way in range(2):
            start = pl.multiple_of(way * SPLIT[0] + core * (SPLIT[way] // 2), 32)
            lines.append(Line(len(lines), c, way, pl.ds(start, SPLIT[way] // 2)))
            lines[-1].kib = SPLIT[way] // 4
    for line in lines:
        source = (wk_hbm, wv_hbm)[line.c].at[line.rows, :]
        line.own = fetch(source, w.at[line.c, zl, y, line.rows, :])
    got_gain = fetch(gain_hbm, gain)
    got_tok = [fetch(tok_hbm.at[s, 0], tok.at[s]) for s in range(4)]
    got_small = [fetch(q_hbm, qv), fetch(hs_hbm, hsv), fetch(ks_hbm, ksv)]

    barrier = pltpu.get_barrier_semaphore()
    friends = [at_z(k) for k in (1, -1, 2, -2)]
    friends += [at_y(k) for k in (1, -1, 2)]
    friends += [at_tp(k) for k in range(1, 8)]
    for friend in friends:
        pl.semaphore_signal(barrier, inc=1, device_id=friend, device_id_type=MESH)
    pl.semaphore_wait(barrier, len(friends))

    every = pl.ds(0, 4)
    side = 1 - 2 * core

    def shift(line, i, j):
        mine = (y, zl) if line.way == 1 else (zl, y)
        return tuple(
            v if k is None else v if isinstance(k, int) and k == 0 else (v + k + 4) % 4
            for v, k in zip(mine, (i, j))
        )

    def pass_on(line, i, j, device, kind):
        a, b = (every if k is None else v for k, v in zip((i, j), shift(line, i, j)))
        if line.way == 1:
            a, b = b, a
        ref = w.at[line.c, a, b, line.rows, :]
        base = line.number * PER_LINE
        send(ref, ref, device, base + SENT, base + kind)

    def arrived(line, kind, pieces):
        take(line.number * PER_LINE + kind, pieces * line.kib)

    def one(line, k):
        return at_y(k) if line.way == 1 else at_z(k)

    def two(line, k):
        return at_z(k) if line.way == 1 else at_y(k)

    def offsets(along_z):
        return (2 * side if along_z else 2, 1, -1)

    def along(line, i):
        for k, kind in zip(offsets(line.way == 1), SECOND):
            pass_on(line, i, 0, two(line, k), kind)

    def wave0(line):
        line.own.wait()
        for k, kind in zip(offsets(line.way == 0), (FAR, NEAR, NEAR)):
            pass_on(line, 0, 0, one(line, k), kind)

    def wave1(line):
        along(line, 0)

    def wave2(line):
        arrived(line, NEAR, 2)
        along(line, -1)
        along(line, 1)

    def wave3(line):
        arrived(line, FAR, 1)
        along(line, 2)
        pass_on(line, None, 0, sibling, PAIR)

    def wave4(line):
        for n, j in ((1, -1), (2, 1), (0, 2)):
            arrived(line, SECOND[n], 4)
            pass_on(line, None, j, sibling, PAIR)

    def wave5(line):
        arrived(line, PAIR, 16)

    def norm(s):
        got_tok[s].wait()

        def block(i, carry):
            for half in range(2):
                r = pl.multiple_of(i * 32 + half * 16, 16)
                rows = pl.ds(r, 16)
                tile = lambda j: tok[s, rows, j * 128 : (j + 1) * 128].astype(F32)
                sums = [tile(j) for j in range(4)]
                for j in range(4, 32):
                    sums[j % 4] = sums[j % 4] + tile(j)
                total = (sums[0] + sums[1]) + (sums[2] + sums[3])
                mean = jnp.sum(total, axis=1, keepdims=True) * (1.0 / D)
                squares = [None] * 4
                for j in range(32):
                    gap = tile(j) - mean
                    old = squares[j % 4]
                    squares[j % 4] = gap * gap if old is None else old + gap * gap
                total = (squares[0] + squares[1]) + (squares[2] + squares[3])
                var = jnp.sum(total, axis=1, keepdims=True) * (1.0 / D)
                scale = lax.rsqrt(var + EPS)
                out_rows = pl.ds(pl.multiple_of(s * 128 + r, 16), 16)
                for j in range(32):
                    cols = slice(j * 128, (j + 1) * 128)
                    value = (tile(j) - mean) * scale * gain[cols].astype(F32).reshape(1, 128)
                    nrm[out_rows, cols] = value.astype(BF16)
            return carry

        lax.fori_loop(0, 4, block, 0)

    lane = lax.broadcasted_iota(jnp.int32, (64, 128), 1)
    left = lane < HD
    left8 = left[:8]

    def turn(v):
        return pltpu.roll(v, HD, 1)

    def project(c):
        acc[...] = jnp.dot(
            nrm[...], w[c].reshape(D, 256), preferred_element_type=F32
        )
        for s in range(4):
            for p in range(2):
                cols = slice(p * 128, (p + 1) * 128)
                top = acc[s * 128 : s * 128 + 64, cols]
                bottom = acc[s * 128 + 64 : s * 128 + 128, cols]
                even = jnp.where(left, top, turn(bottom))
                odd = jnp.where(left, turn(top), bottom)
                kvs[c, s * 4 + 2 * p] = even.astype(BF16)
                kvs[c, s * 4 + 2 * p + 1] = odd.astype(BF16)
        kvr[c, sp] = kvs[c, sp]
        for k in range(1, 16):
            far = at_sp(k)
            send(kvs.at[c, far[1]], kvr.at[c, sp], far, BLOCKS_SENT + c, BLOCKS + c)

    k_lines = [line for line in lines if line.c == 0]
    v_lines = [line for line in lines if line.c == 1]

    def each(wave, some):
        for line in some:
            wave(line)

    each(wave0, k_lines)
    each(wave0, v_lines)
    got_gain.wait()
    norm(0)
    each(wave1, k_lines)
    each(wave2, k_lines)
    each(wave3, k_lines)
    each(wave1, v_lines)
    each(wave2, v_lines)
    each(wave3, v_lines)
    norm(1)
    norm(2)
    norm(3)
    each(wave4, k_lines)
    each(wave5, k_lines)
    project(0)
    each(wave4, v_lines)
    each(wave5, v_lines)
    project(1)

    for copy in got_small:
        copy.wait()
    row8 = lax.broadcasted_iota(jnp.int32, (8, 128), 0)
    qq = jnp.zeros((8, 128), F32)
    for g in range(GROUP):
        part = qv[:, (g // 2) * 128 : (g // 2 + 1) * 128].astype(F32)
        part = jnp.broadcast_to(part, (8, 128))
        other = turn(part)
        mine = jnp.where(left8, part, other) if g % 2 == 0 else jnp.where(left8, other, part)
        qq = jnp.where(row8 == g, mine, qq)
    q_lo = jnp.where(left8, qq, 0.0)
    q_hi = jnp.where(left8, 0.0, qq)
    stack = jnp.concatenate([q_lo, q_hi], axis=0).astype(BF16)
    hrow = lax.broadcasted_iota(jnp.int32, (4, 8), 0)
    own = jnp.sum(jnp.where(hrow == y, hsv[...], 0.0), axis=0, keepdims=True)
    eye = lax.broadcasted_iota(jnp.int32, (8, 8), 0) == lax.broadcasted_iota(jnp.int32, (8, 8), 1)
    head = jnp.sum(jnp.where(eye, jnp.broadcast_to(own, (8, 8)), 0.0), axis=1, keepdims=True)

    take(BLOCKS, 240)
    logits = lax.dot_general(
        stack, kvr[0].reshape(1024, 128), (((1,), (1,)), ((), ())), preferred_element_type=F32
    )
    tiles = []
    for m in range(8):
        cols = slice(m * 128, (m + 1) * 128)
        lo, hi = logits[:8, cols], logits[8:, cols]
        tiles.append(jnp.where(left8, lo, turn(hi)))
        tiles.append(jnp.where(left8, turn(lo), hi))
    z_all = jnp.concatenate(
        [
            t * HD ** (-0.5) + head + ksv[:, n * 128 : (n + 1) * 128]
            for n, t in enumerate(tiles)
        ],
        axis=0,
    )
    log_beta = jnp.minimum(z_all, 0.0) - jnp.log1p(jnp.exp(-jnp.abs(z_all)))
    log_keep = log_beta - z_all
    ri = lax.broadcasted_iota(jnp.int32, (128, 256), 0)
    ci = lax.broadcasted_iota(jnp.int32, (128, 256), 1)
    later = jnp.where((ci >= 128) | (ri > ci), 1.0, 0.0).astype(F32)
    sums = jnp.dot(
        log_keep, later, preferred_element_type=F32, precision=lax.Precision.HIGHEST
    )
    tail = jnp.zeros((8, 128), F32)
    weights = [None] * 16
    for n in reversed(range(16)):
        rows = slice(n * 8, (n + 1) * 8)
        weights[n] = jnp.exp(log_beta[rows] + (sums[rows, :128] + tail))
        tail = tail + sums[rows, 128:]
    w_lo = [jnp.where(left8, weights[2 * m], turn(weights[2 * m + 1])) for m in range(8)]
    w_hi = [jnp.where(left8, turn(weights[2 * m]), weights[2 * m + 1]) for m in range(8)]
    wstack = jnp.concatenate(
        [jnp.concatenate(w_lo, axis=1), jnp.concatenate(w_hi, axis=1)], axis=0
    ).astype(BF16)

    take(BLOCKS + 1, 240)
    out = jnp.dot(wstack, kvr[1].reshape(1024, 128), preferred_element_type=F32)
    section = out[:8] + turn(out[8:])
    message = jnp.where(left8, section, tail)
    xs[...] = message
    xr[tp] = message
    for k in range(1, 8):
        send(xs, xr.at[tp], at_tp(k), SHARED_SENT, SHARED)

    def assemble(j, carry):
        keys = kvr[0, j].astype(F32)
        values = kvr[1, j].astype(F32)
        first = pl.multiple_of(j * 128, 64)
        second = pl.multiple_of(j * 128 + 64, 64)
        cache[pl.ds(first, 64), :] = jnp.where(left, keys, turn(values)).astype(BF16)
        cache[pl.ds(second, 64), :] = jnp.where(left, turn(keys), values).astype(BF16)
        return carry

    lax.fori_loop(0, 16, assemble, 0)
    stored = fetch(cache, cache_hbm.at[0])

    take(SHARED, 28)
    carry = jnp.zeros((8, 128), F32)
    result = jnp.zeros((8, 128), F32)
    for t in reversed(range(8)):
        tile = xr[t]
        result = result + jnp.exp(carry) * tile
        carry = carry + turn(tile)
    result = jnp.where(left8, result, turn(result))
    for k in range(4):
        rdv[:, k * 128 : (k + 1) * 128] = jnp.where(
            left8[:1], result[2 * k : 2 * k + 1], result[2 * k + 1 : 2 * k + 2]
        )
    answered = fetch(rdv, read_hbm)
    for line in lines:
        take(line.number * PER_LINE + SENT, 31 * line.kib)
    for c in range(2):
        take(BLOCKS_SENT + c, 240)
    take(SHARED_SENT, 28)
    stored.wait()
    answered.wait()


def local(tokens, ln_gain, w_key, w_value, queries, head_shift, key_shift):
    any_ = pl.BlockSpec(memory_space=pl.ANY)
    return pl.pallas_call(
        kernel,
        out_shape=(
            jax.ShapeDtypeStruct((1, 2048, 128), BF16),
            jax.ShapeDtypeStruct((1, 512), F32),
        ),
        in_specs=[any_] * 7,
        out_specs=(any_, any_),
        scratch_shapes=[
            pltpu.VMEM((4, 128, D), BF16),
            pltpu.VMEM((512, D), BF16),
            pltpu.VMEM((2, 4, 4, 256, 256), BF16),
            pltpu.VMEM((512, 256), F32),
            pltpu.VMEM((2, 16, 64, 128), BF16),
            pltpu.VMEM((2, 16, 64, 128), BF16),
            pltpu.VMEM((2048, 128), BF16),
            pltpu.VMEM((D,), BF16),
            pltpu.VMEM((1, 512), BF16),
            pltpu.VMEM((4, 8), F32),
            pltpu.VMEM((1, 2048), F32),
            pltpu.VMEM((1, 512), F32),
            pltpu.VMEM((8, 128), F32),
            pltpu.VMEM((8, 8, 128), F32),
            pltpu.VMEM((4096, 128), BF16),
            pltpu.SemaphoreType.DMA((14,)),
            pltpu.SemaphoreType.DMA((SEMAPHORES,)),
        ],
        compiler_params=pltpu.CompilerParams(collective_id=0, has_side_effects=True),
    )(tokens, ln_gain, w_key, w_value, queries, head_shift, key_shift)


def solution(mesh):
    placed = (
        P("gr", "tp", "sp", None),
        P(),
        P("sp", None),
        P("sp", None),
        P(("gr", "sp"), None),
        P(),
        P(("gr", "sp"), "tp"),
    )
    return jax.shard_map(
        local,
        mesh=mesh,
        in_specs=placed,
        out_specs=(P(("gr", "sp"), "tp", None), P(("gr", "sp"), None)),
        check_vma=False,
    )
```

```python
import functools

import jax
import jax.numpy as jnp
from jax import lax
from jax.experimental import pallas as pl
from jax.experimental.pallas import tpu as pltpu
from jax.sharding import PartitionSpec as P

MESH = pl.DeviceIdType.MESH
F32, BF16 = jnp.float32, jnp.bfloat16
D, HD, KVH, GROUP = 4096, 64, 4, 8
EPS = 1e-05
SPLIT = (128, 128)
LINES, PER_LINE = 4, 8
NEAR, FAR, SECOND, PAIR, SENT, LATE = 0, 1, (2, 3, 4), 5, 6, 7
BLOCKS, BLOCKS_SENT = LINES * PER_LINE, LINES * PER_LINE + 2
SHARED, SHARED_SENT = BLOCKS + 4, BLOCKS + 5
SEMAPHORES = BLOCKS + 6


class Line:
    def __init__(self, number, c, way, rows):
        self.number, self.c, self.way, self.rows = number, c, way, rows


def kernel(
    tok_hbm, gain_hbm, wk_hbm, wv_hbm, q_hbm, hs_hbm, ks_hbm,
    cache_hbm, xr,
    tok, nrm, w, acc, kvs, kvr, cache, gain, qv, hsv, ksv, xs,
    ruler, local_sem, sems,
):
    gr, sp, tp = lax.axis_index("gr"), lax.axis_index("sp"), lax.axis_index("tp")
    x, core = tp // 2, tp % 2
    zl, y = sp // 4, sp % 4
    z = gr * 4 + zl

    def at_z(k):
        far = (z + k) % 8
        return (far // 4, (far % 4) * 4 + y, tp)

    def at_y(k):
        return (gr, zl * 4 + (y + k) % 4, tp)

    def at_sp(k):
        return (gr, (sp + k) % 16, tp)

    def at_tp(k):
        return (gr, sp, (tp + k) % 8)

    sibling = (gr, sp, x * 2 + 1 - core)

    def send(src, dst, device, sent, arrived):
        pltpu.make_async_remote_copy(
            src_ref=src,
            dst_ref=dst,
            send_sem=sems.at[sent],
            recv_sem=sems.at[arrived],
            device_id=device,
            device_id_type=MESH,
        ).start()

    def take(number, kib):
        span = ruler.at[pl.ds(0, kib * 4), :]
        pltpu.make_async_copy(span, span, sems.at[number]).wait()

    locals_ = []

    def fetch(src, dst):
        copy = pltpu.make_async_copy(src, dst, local_sem.at[len(locals_)])
        copy.start()
        locals_.append(copy)
        return copy

    lines = []
    for c in range(2):
        for way in range(2):
            start = pl.multiple_of(way * SPLIT[0] + core * (SPLIT[way] // 2), 32)
            lines.append(Line(len(lines), c, way, pl.ds(start, SPLIT[way] // 2)))
            lines[-1].kib = SPLIT[way] // 4
    for line in lines:
        source = (wk_hbm, wv_hbm)[line.c].at[line.rows, :]
        line.own = fetch(source, w.at[line.c, zl, y, line.rows, :])
    got_gain = fetch(gain_hbm, gain)
    got_tok = [fetch(tok_hbm.at[s, 0], tok.at[s]) for s in range(4)]
    got_small = [fetch(q_hbm, qv), fetch(hs_hbm, hsv), fetch(ks_hbm, ksv)]

    barrier = pltpu.get_barrier_semaphore()
    friends = [at_z(k) for k in (1, -1, 2, -2)]
    friends += [at_y(k) for k in (1, -1, 2)]
    friends += [at_tp(k) for k in range(1, 8)]
    for friend in friends:
        pl.semaphore_signal(barrier, inc=1, device_id=friend, device_id_type=MESH)
    pl.semaphore_wait(barrier, len(friends))

    every = pl.ds(0, 4)
    side = 1 - 2 * core

    def shift(line, i, j):
        mine = (y, zl) if line.way == 1 else (zl, y)
        return tuple(
            v if k is None else v if isinstance(k, int) and k == 0 else (v + k + 4) % 4
            for v, k in zip(mine, (i, j))
        )

    def pass_on(line, i, j, device, kind):
        a, b = (every if k is None else v for k, v in zip((i, j), shift(line, i, j)))
        if line.way == 1:
            a, b = b, a
        ref = w.at[line.c, a, b, line.rows, :]
        base = line.number * PER_LINE
        send(ref, ref, device, base + SENT, base + kind)

    def arrived(line, kind, pieces):
        take(line.number * PER_LINE + kind, pieces * line.kib)

    def one(line, k):
        return at_y(k) if line.way == 1 else at_z(k)

    def two(line, k):
        return at_z(k) if line.way == 1 else at_y(k)

    def offsets(along_z):
        return (2 * side if along_z else 2, 1, -1)

    def along(line, i):
        for k, kind in zip(offsets(line.way == 1), SECOND):
            pass_on(line, i, 0, two(line, k), LATE if i == 2 else kind)

    def wave0(line):
        line.own.wait()
        for k, kind in zip(offsets(line.way == 0), (FAR, NEAR, NEAR)):
            pass_on(line, 0, 0, one(line, k), kind)

    def wave1(line):
        along(line, 0)

    def wave2(line):
        arrived(line, NEAR, 2)
        along(line, -1)
        along(line, 1)

    def wave3(line):
        arrived(line, FAR, 1)
        along(line, 2)
        pass_on(line, None, 0, sibling, PAIR)

    def wave4(line):
        for n, j in ((1, -1), (2, 1), (0, 2)):
            arrived(line, SECOND[n], 3)
            for i in (0, -1, 1):
                pass_on(line, i, j, sibling, PAIR)

    def wave6(line):
        arrived(line, LATE, 3)
        for j in (-1, 1, 2):
            pass_on(line, 2, j, sibling, PAIR)

    def wave5(line):
        arrived(line, PAIR, 16)

    def norm(s):
        got_tok[s].wait()

        def block(i, carry):
            for half in range(2):
                r = pl.multiple_of(i * 32 + half * 16, 16)
                rows = pl.ds(r, 16)
                tile = lambda j: tok[s, rows, j * 128 : (j + 1) * 128].astype(F32)
                sums = [tile(j) for j in range(4)]
                for j in range(4, 32):
                    sums[j % 4] = sums[j % 4] + tile(j)
                total = (sums[0] + sums[1]) + (sums[2] + sums[3])
                mean = jnp.sum(total, axis=1, keepdims=True) * (1.0 / D)
                squares = [None] * 4
                for j in range(32):
                    gap = tile(j) - mean
                    old = squares[j % 4]
                    squares[j % 4] = gap * gap if old is None else old + gap * gap
                total = (squares[0] + squares[1]) + (squares[2] + squares[3])
                var = jnp.sum(total, axis=1, keepdims=True) * (1.0 / D)
                scale = lax.rsqrt(var + EPS)
                out_rows = pl.ds(pl.multiple_of(s * 128 + r, 16), 16)
                for j in range(32):
                    cols = slice(j * 128, (j + 1) * 128)
                    value = (tile(j) - mean) * scale * gain[cols].astype(F32).reshape(1, 128)
                    nrm[out_rows, cols] = value.astype(BF16)
            return carry

        lax.fori_loop(0, 4, block, 0)

    lane = lax.broadcasted_iota(jnp.int32, (64, 128), 1)
    left = lane < HD
    left8 = left[:8]

    def turn(v):
        return pltpu.roll(v, HD, 1)

    def project(c):
        acc[...] = jnp.dot(
            nrm[...], w[c].reshape(D, 256), preferred_element_type=F32
        )
        for s in range(4):
            for p in range(2):
                cols = slice(p * 128, (p + 1) * 128)
                top = acc[s * 128 : s * 128 + 64, cols]
                bottom = acc[s * 128 + 64 : s * 128 + 128, cols]
                even = jnp.where(left, top, turn(bottom))
                odd = jnp.where(left, turn(top), bottom)
                kvs[c, s * 4 + 2 * p] = even.astype(BF16)
                kvs[c, s * 4 + 2 * p + 1] = odd.astype(BF16)
        kvr[c, sp] = kvs[c, sp]
        for k in range(1, 16):
            far = at_sp(k)
            send(kvs.at[c, far[1]], kvr.at[c, sp], far, BLOCKS_SENT + c, BLOCKS + c)

    k_lines = [line for line in lines if line.c == 0]
    v_lines = [line for line in lines if line.c == 1]

    def each(wave, some):
        for line in some:
            wave(line)

    each(wave0, k_lines)
    each(wave0, v_lines)
    got_gain.wait()
    norm(0)
    each(wave1, k_lines)
    each(wave2, k_lines)
    each(wave3, k_lines)
    each(wave1, v_lines)
    each(wave2, v_lines)
    each(wave3, v_lines)
    norm(1)
    norm(2)
    each(wave4, k_lines)
    norm(3)
    each(wave6, k_lines)
    each(wave5, k_lines)
    project(0)
    each(wave4, v_lines)
    each(wave6, v_lines)
    each(wave5, v_lines)
    project(1)

    for copy in got_small:
        copy.wait()
    row8 = lax.broadcasted_iota(jnp.int32, (8, 128), 0)
    qq = jnp.zeros((8, 128), F32)
    for g in range(GROUP):
        part = qv[:, (g // 2) * 128 : (g // 2 + 1) * 128].astype(F32)
        part = jnp.broadcast_to(part, (8, 128))
        other = turn(part)
        mine = jnp.where(left8, part, other) if g % 2 == 0 else jnp.where(left8, other, part)
        qq = jnp.where(row8 == g, mine, qq)
    q_lo = jnp.where(left8, qq, 0.0)
    q_hi = jnp.where(left8, 0.0, qq)
    stack = jnp.concatenate([q_lo, q_hi], axis=0).astype(BF16)
    hrow = lax.broadcasted_iota(jnp.int32, (4, 8), 0)
    own = jnp.sum(jnp.where(hrow == y, hsv[...], 0.0), axis=0, keepdims=True)
    eye = lax.broadcasted_iota(jnp.int32, (8, 8), 0) == lax.broadcasted_iota(jnp.int32, (8, 8), 1)
    head = jnp.sum(jnp.where(eye, jnp.broadcast_to(own, (8, 8)), 0.0), axis=1, keepdims=True)

    take(BLOCKS, 240)
    logits = lax.dot_general(
        stack, kvr[0].reshape(1024, 128), (((1,), (1,)), ((), ())), preferred_element_type=F32
    )
    tiles = []
    for m in range(8):
        cols = slice(m * 128, (m + 1) * 128)
        lo, hi = logits[:8, cols], logits[8:, cols]
        tiles.append(jnp.where(left8, lo, turn(hi)))
        tiles.append(jnp.where(left8, turn(lo), hi))
    z_all = jnp.concatenate(
        [
            t * HD ** (-0.5) + head + ksv[:, n * 128 : (n + 1) * 128]
            for n, t in enumerate(tiles)
        ],
        axis=0,
    )
    log_beta = jnp.minimum(z_all, 0.0) - jnp.log1p(jnp.exp(-jnp.abs(z_all)))
    log_keep = log_beta - z_all
    ri = lax.broadcasted_iota(jnp.int32, (128, 256), 0)
    ci = lax.broadcasted_iota(jnp.int32, (128, 256), 1)
    later = jnp.where((ci >= 128) | (ri > ci), 1.0, 0.0).astype(F32)
    sums = jnp.dot(
        log_keep, later, preferred_element_type=F32, precision=lax.Precision.HIGHEST
    )
    tail = jnp.zeros((8, 128), F32)
    weights = [None] * 16
    for n in reversed(range(16)):
        rows = slice(n * 8, (n + 1) * 8)
        weights[n] = jnp.exp(log_beta[rows] + (sums[rows, :128] + tail))
        tail = tail + sums[rows, 128:]
    w_lo = [jnp.where(left8, weights[2 * m], turn(weights[2 * m + 1])) for m in range(8)]
    w_hi = [jnp.where(left8, turn(weights[2 * m]), weights[2 * m + 1]) for m in range(8)]
    wstack = jnp.concatenate(
        [jnp.concatenate(w_lo, axis=1), jnp.concatenate(w_hi, axis=1)], axis=0
    ).astype(BF16)

    take(BLOCKS + 1, 240)
    out = jnp.dot(wstack, kvr[1].reshape(1024, 128), preferred_element_type=F32)
    section = out[:8] + turn(out[8:])
    message = jnp.where(left8, section, tail)
    xs[...] = message
    kept = fetch(xs, xr.at[tp])
    for k in range(1, 8):
        send(xs, xr.at[tp], at_tp(k), SHARED_SENT, SHARED)

    def assemble(j, carry):
        keys = kvr[0, j].astype(F32)
        values = kvr[1, j].astype(F32)
        first = pl.multiple_of(j * 128, 64)
        second = pl.multiple_of(j * 128 + 64, 64)
        cache[pl.ds(first, 64), :] = jnp.where(left, keys, turn(values)).astype(BF16)
        cache[pl.ds(second, 64), :] = jnp.where(left, turn(keys), values).astype(BF16)
        return carry

    lax.fori_loop(0, 16, assemble, 0)
    stored = fetch(cache, cache_hbm.at[0])

    take(SHARED, 28)
    for line in lines:
        take(line.number * PER_LINE + SENT, 31 * line.kib)
    for c in range(2):
        take(BLOCKS_SENT + c, 240)
    take(SHARED_SENT, 28)
    stored.wait()
    kept.wait()


def write_out(cache_in, shared_in, cache_out, read_out, cache, xr, rdv, sems):
    shared = pltpu.make_async_copy(shared_in, xr, sems.at[0, 4])
    shared.start()
    ways = [
        tuple(ref.at[pl.ds(k * 512, 512)] for ref in (cache_in.at[0], cache, cache_out.at[0]))
        for k in range(4)
    ]
    reads = [pltpu.make_async_copy(a, b, sems.at[0, n]) for n, (a, b, _) in enumerate(ways)]
    writes = [pltpu.make_async_copy(b, c, sems.at[1, n]) for n, (_, b, c) in enumerate(ways)]
    for copy in reads:
        copy.start()
    left8 = lax.broadcasted_iota(jnp.int32, (8, 128), 1) < HD
    turn = lambda v: pltpu.roll(v, HD, 1)
    shared.wait()
    carry = jnp.zeros((8, 128), F32)
    result = jnp.zeros((8, 128), F32)
    for t in reversed(range(8)):
        tile = xr[t]
        result = result + jnp.exp(carry) * tile
        carry = carry + turn(tile)
    result = jnp.where(left8, result, turn(result))
    for k in range(4):
        rdv[:, k * 128 : (k + 1) * 128] = jnp.where(
            left8[:1], result[2 * k : 2 * k + 1], result[2 * k + 1 : 2 * k + 2]
        )
    answered = pltpu.make_async_copy(rdv, read_out, sems.at[1, 4])
    answered.start()
    for before, after in zip(reads, writes):
        before.wait()
        after.start()
    for copy in writes:
        copy.wait()
    answered.wait()


def local(tokens, ln_gain, w_key, w_value, queries, head_shift, key_shift):
    any_ = pl.BlockSpec(memory_space=pl.ANY)
    cache, shared = pl.pallas_call(
        kernel,
        out_shape=(
            jax.ShapeDtypeStruct((1, 2048, 128), BF16),
            jax.ShapeDtypeStruct((8, 8, 128), F32),
        ),
        in_specs=[any_] * 7,
        out_specs=(any_, any_),
        scratch_shapes=[
            pltpu.VMEM((4, 128, D), BF16),
            pltpu.VMEM((512, D), BF16),
            pltpu.VMEM((2, 4, 4, 256, 256), BF16),
            pltpu.VMEM((512, 256), F32),
            pltpu.VMEM((2, 16, 64, 128), BF16),
            pltpu.VMEM((2, 16, 64, 128), BF16),
            pltpu.VMEM((2048, 128), BF16),
            pltpu.VMEM((D,), BF16),
            pltpu.VMEM((1, 512), BF16),
            pltpu.VMEM((4, 8), F32),
            pltpu.VMEM((1, 2048), F32),
            pltpu.VMEM((8, 128), F32),
            pltpu.VMEM((4096, 128), BF16),
            pltpu.SemaphoreType.DMA((14,)),
            pltpu.SemaphoreType.DMA((SEMAPHORES,)),
        ],
        compiler_params=pltpu.CompilerParams(collective_id=0, has_side_effects=True),
    )(tokens, ln_gain, w_key, w_value, queries, head_shift, key_shift)
    return pl.pallas_call(
        write_out,
        out_shape=(
            jax.ShapeDtypeStruct((1, 2048, 128), BF16),
            jax.ShapeDtypeStruct((1, 512), F32),
        ),
        in_specs=[any_] * 2,
        out_specs=(any_, any_),
        scratch_shapes=[
            pltpu.VMEM((2048, 128), BF16),
            pltpu.VMEM((8, 8, 128), F32),
            pltpu.VMEM((1, 512), F32),
            pltpu.SemaphoreType.DMA((2, 5)),
        ],
    )(cache, shared)


def solution(mesh):
    placed = (
        P("gr", "tp", "sp", None),
        P(),
        P("sp", None),
        P("sp", None),
        P(("gr", "sp"), None),
        P(),
        P(("gr", "sp"), "tp"),
    )
    return jax.shard_map(
        local,
        mesh=mesh,
        in_specs=placed,
        out_specs=(P(("gr", "sp"), "tp", None), P(("gr", "sp"), None)),
        check_vma=False,
    )
```

```python
import functools

import jax
import jax.numpy as jnp
from jax import lax
from jax.experimental import pallas as pl
from jax.experimental.pallas import tpu as pltpu
from jax.sharding import PartitionSpec as P

MESH = pl.DeviceIdType.MESH
F32, BF16 = jnp.float32, jnp.bfloat16
D, HD, KVH, GROUP = 4096, 64, 4, 8
EPS = 1e-05
SPLIT = (128, 128)
LINES, PER_LINE = 4, 8
NEAR, FAR, SECOND, PAIR, SENT, LATE = 0, 1, (2, 3, 4), 5, 6, 7
BLOCKS, BLOCKS_SENT = LINES * PER_LINE, LINES * PER_LINE + 2
SHARED, SHARED_SENT = BLOCKS + 4, BLOCKS + 5
SEMAPHORES = BLOCKS + 6
GROUPS = ((2, 3), (1, 0))


class Line:
    def __init__(self, number, c, way, rows):
        self.number, self.c, self.way, self.rows = number, c, way, rows


def kernel(
    tok_hbm, gain_hbm, wk_hbm, wv_hbm, q_hbm, hs_hbm, ks_hbm,
    cache_hbm, xr,
    tok, nrm, w, acc, kvs, kvr, cache, gain, qv, hsv, ksv, xs,
    ruler, local_sem, sems,
):
    gr, sp, tp = lax.axis_index("gr"), lax.axis_index("sp"), lax.axis_index("tp")
    x, core = tp // 2, tp % 2
    zl, y = sp // 4, sp % 4
    z = gr * 4 + zl

    def at_z(k):
        far = (z + k) % 8
        return (far // 4, (far % 4) * 4 + y, tp)

    def at_y(k):
        return (gr, zl * 4 + (y + k) % 4, tp)

    def at_sp(k):
        return (gr, (sp + k) % 16, tp)

    def at_tp(k):
        return (gr, sp, (tp + k) % 8)

    sibling = (gr, sp, x * 2 + 1 - core)

    def send(src, dst, device, sent, arrived):
        pltpu.make_async_remote_copy(
            src_ref=src,
            dst_ref=dst,
            send_sem=sems.at[sent],
            recv_sem=sems.at[arrived],
            device_id=device,
            device_id_type=MESH,
        ).start()

    def take(number, kib):
        span = ruler.at[pl.ds(0, kib * 4), :]
        pltpu.make_async_copy(span, span, sems.at[number]).wait()

    locals_ = []

    def fetch(src, dst):
        copy = pltpu.make_async_copy(src, dst, local_sem.at[len(locals_)])
        copy.start()
        locals_.append(copy)
        return copy

    barrier = pltpu.get_barrier_semaphore()
    friends = [at_z(k) for k in (1, -1, 2, -2)]
    friends += [at_y(k) for k in (1, -1, 2)]
    friends += [at_tp(k) for k in range(1, 8)]
    for friend in friends:
        pl.semaphore_signal(barrier, inc=1, device_id=friend, device_id_type=MESH)

    lines = []
    for c in range(2):
        for way in range(2):
            start = pl.multiple_of(way * SPLIT[0] + core * (SPLIT[way] // 2), 32)
            lines.append(Line(len(lines), c, way, pl.ds(start, SPLIT[way] // 2)))
            lines[-1].kib = SPLIT[way] // 4
    for line in lines:
        source = (wk_hbm, wv_hbm)[line.c].at[line.rows, :]
        line.own = fetch(source, w.at[line.c, zl, y, line.rows, :])
    got_gain = fetch(gain_hbm, gain)
    got_tok = [fetch(tok_hbm.at[s, 0], tok.at[s]) for s in range(4)]
    got_small = [fetch(q_hbm, qv), fetch(hs_hbm, hsv), fetch(ks_hbm, ksv)]

    pl.semaphore_wait(barrier, len(friends))

    every = pl.ds(0, 4)
    side = 1 - 2 * core

    def shift(line, i, j):
        mine = (y, zl) if line.way == 1 else (zl, y)
        return tuple(
            v if k is None else v if isinstance(k, int) and k == 0 else (v + k + 4) % 4
            for v, k in zip(mine, (i, j))
        )

    def pass_on(line, i, j, device, kind):
        a, b = (every if k is None else v for k, v in zip((i, j), shift(line, i, j)))
        if line.way == 1:
            a, b = b, a
        ref = w.at[line.c, a, b, line.rows, :]
        base = line.number * PER_LINE
        send(ref, ref, device, base + SENT, base + kind)

    def arrived(line, kind, pieces):
        take(line.number * PER_LINE + kind, pieces * line.kib)

    def one(line, k):
        return at_y(k) if line.way == 1 else at_z(k)

    def two(line, k):
        return at_z(k) if line.way == 1 else at_y(k)

    def offsets(along_z):
        return (2 * side if along_z else 2, 1, -1)

    def along(line, i):
        for k, kind in zip(offsets(line.way == 1), SECOND):
            pass_on(line, i, 0, two(line, k), LATE if i == 2 else kind)

    def wave0(line):
        line.own.wait()
        for k, kind in zip(offsets(line.way == 0), (FAR, NEAR, NEAR)):
            pass_on(line, 0, 0, one(line, k), kind)

    def wave1(line):
        along(line, 0)

    def wave2(line):
        arrived(line, NEAR, 2)
        along(line, -1)
        along(line, 1)

    def wave3(line):
        arrived(line, FAR, 1)
        along(line, 2)
        pass_on(line, None, 0, sibling, PAIR)

    def wave4(line):
        for n, j in ((1, -1), (2, 1), (0, 2)):
            arrived(line, SECOND[n], 3)
            for i in (0, -1, 1):
                pass_on(line, i, j, sibling, PAIR)

    def wave6(line):
        arrived(line, LATE, 3)
        for j in (-1, 1, 2):
            pass_on(line, 2, j, sibling, PAIR)

    def wave5(line):
        arrived(line, PAIR, 16)

    def norm(s):
        got_tok[s].wait()

        def block(i, carry):
            for half in range(2):
                r = pl.multiple_of(i * 32 + half * 16, 16)
                rows = pl.ds(r, 16)
                tile = lambda j: tok[s, rows, j * 128 : (j + 1) * 128].astype(F32)
                sums = [tile(j) for j in range(4)]
                for j in range(4, 32):
                    sums[j % 4] = sums[j % 4] + tile(j)
                total = (sums[0] + sums[1]) + (sums[2] + sums[3])
                mean = jnp.sum(total, axis=1, keepdims=True) * (1.0 / D)
                squares = [None] * 4
                for j in range(32):
                    gap = tile(j) - mean
                    old = squares[j % 4]
                    squares[j % 4] = gap * gap if old is None else old + gap * gap
                total = (squares[0] + squares[1]) + (squares[2] + squares[3])
                var = jnp.sum(total, axis=1, keepdims=True) * (1.0 / D)
                scale = lax.rsqrt(var + EPS)
                out_rows = pl.ds(pl.multiple_of(s * 128 + r, 16), 16)
                for j in range(32):
                    cols = slice(j * 128, (j + 1) * 128)
                    value = (tile(j) - mean) * scale * gain[cols].astype(F32).reshape(1, 128)
                    nrm[out_rows, cols] = value.astype(BF16)
            return carry

        lax.fori_loop(0, 4, block, 0)

    lane = lax.broadcasted_iota(jnp.int32, (64, 128), 1)
    left = lane < HD
    left8 = left[:8]

    def turn(v):
        return pltpu.roll(v, HD, 1)

    def project(c):
        weights = w[c].reshape(D, 256)
        for group in GROUPS:
            starts = [(zl + o) % 4 for o in group]
            rows = [nrm[pl.ds(pl.multiple_of(s * 128, 128), 128), :] for s in starts]
            acc[: len(group) * 128] = jnp.dot(
                jnp.concatenate(rows, axis=0), weights, preferred_element_type=F32
            )
            for n, (o, s) in enumerate(zip(group, starts)):
                for p in range(2):
                    cols = slice(p * 128, (p + 1) * 128)
                    top = acc[n * 128 : n * 128 + 64, cols]
                    bottom = acc[n * 128 + 64 : n * 128 + 128, cols]
                    even = jnp.where(left, top, turn(bottom))
                    odd = jnp.where(left, turn(top), bottom)
                    kvs[c, s * 4 + 2 * p] = even.astype(BF16)
                    kvs[c, s * 4 + 2 * p + 1] = odd.astype(BF16)
                for k in range(4):
                    far = s * 4 + (y + k) % 4
                    if o or k:
                        device = (gr, far, tp)
                        send(kvs.at[c, far], kvr.at[c, sp], device, BLOCKS_SENT + c, BLOCKS + c)
                    else:
                        kvr[c, sp] = kvs[c, sp]

    k_lines = [line for line in lines if line.c == 0]
    v_lines = [line for line in lines if line.c == 1]

    def each(wave, some):
        for line in some:
            wave(line)

    each(wave0, k_lines)
    each(wave0, v_lines)
    got_gain.wait()
    norm(0)
    each(wave1, k_lines)
    each(wave2, k_lines)
    each(wave3, k_lines)
    each(wave1, v_lines)
    each(wave2, v_lines)
    each(wave3, v_lines)
    norm(1)
    norm(2)
    each(wave4, k_lines)
    norm(3)
    each(wave6, k_lines)
    each(wave5, k_lines)
    project(0)
    each(wave4, v_lines)
    each(wave6, v_lines)
    each(wave5, v_lines)
    project(1)

    for copy in got_small:
        copy.wait()
    row8 = lax.broadcasted_iota(jnp.int32, (8, 128), 0)
    qq = jnp.zeros((8, 128), F32)
    for g in range(GROUP):
        part = qv[:, (g // 2) * 128 : (g // 2 + 1) * 128].astype(F32)
        part = jnp.broadcast_to(part, (8, 128))
        other = turn(part)
        mine = jnp.where(left8, part, other) if g % 2 == 0 else jnp.where(left8, other, part)
        qq = jnp.where(row8 == g, mine, qq)
    q_lo = jnp.where(left8, qq, 0.0)
    q_hi = jnp.where(left8, 0.0, qq)
    stack = jnp.concatenate([q_lo, q_hi], axis=0).astype(BF16)
    hrow = lax.broadcasted_iota(jnp.int32, (4, 8), 0)
    own = jnp.sum(jnp.where(hrow == y, hsv[...], 0.0), axis=0, keepdims=True)
    eye = lax.broadcasted_iota(jnp.int32, (8, 8), 0) == lax.broadcasted_iota(jnp.int32, (8, 8), 1)
    head = jnp.sum(jnp.where(eye, jnp.broadcast_to(own, (8, 8)), 0.0), axis=1, keepdims=True)

    take(BLOCKS, 240)
    logits = lax.dot_general(
        stack, kvr[0].reshape(1024, 128), (((1,), (1,)), ((), ())), preferred_element_type=F32
    )
    tiles = []
    for m in range(8):
        cols = slice(m * 128, (m + 1) * 128)
        lo, hi = logits[:8, cols], logits[8:, cols]
        tiles.append(jnp.where(left8, lo, turn(hi)))
        tiles.append(jnp.where(left8, turn(lo), hi))
    z_all = jnp.concatenate(
        [
            t * HD ** (-0.5) + head + ksv[:, n * 128 : (n + 1) * 128]
            for n, t in enumerate(tiles)
        ],
        axis=0,
    )
    log_beta = jnp.minimum(z_all, 0.0) - jnp.log1p(jnp.exp(-jnp.abs(z_all)))
    log_keep = log_beta - z_all
    ri = lax.broadcasted_iota(jnp.int32, (128, 256), 0)
    ci = lax.broadcasted_iota(jnp.int32, (128, 256), 1)
    later = jnp.where((ci >= 128) | (ri > ci), 1.0, 0.0).astype(F32)
    sums = jnp.dot(
        log_keep, later, preferred_element_type=F32, precision=lax.Precision.HIGHEST
    )
    tail = jnp.zeros((8, 128), F32)
    weights = [None] * 16
    for n in reversed(range(16)):
        rows = slice(n * 8, (n + 1) * 8)
        weights[n] = jnp.exp(log_beta[rows] + (sums[rows, :128] + tail))
        tail = tail + sums[rows, 128:]
    w_lo = [jnp.where(left8, weights[2 * m], turn(weights[2 * m + 1])) for m in range(8)]
    w_hi = [jnp.where(left8, turn(weights[2 * m]), weights[2 * m + 1]) for m in range(8)]
    wstack = jnp.concatenate(
        [jnp.concatenate(w_lo, axis=1), jnp.concatenate(w_hi, axis=1)], axis=0
    ).astype(BF16)

    take(BLOCKS + 1, 240)
    out = jnp.dot(wstack, kvr[1].reshape(1024, 128), preferred_element_type=F32)
    section = out[:8] + turn(out[8:])
    message = jnp.where(left8, section, tail)
    xs[...] = message
    kept = fetch(xs, xr.at[tp])
    for k in range(1, 8):
        send(xs, xr.at[tp], at_tp(k), SHARED_SENT, SHARED)

    def assemble(j, carry):
        keys = kvr[0, j].astype(F32)
        values = kvr[1, j].astype(F32)
        first = pl.multiple_of(j * 128, 64)
        second = pl.multiple_of(j * 128 + 64, 64)
        cache[pl.ds(first, 64), :] = jnp.where(left, keys, turn(values)).astype(BF16)
        cache[pl.ds(second, 64), :] = jnp.where(left, turn(keys), values).astype(BF16)
        return carry

    lax.fori_loop(0, 16, assemble, 0)
    stored = fetch(cache, cache_hbm.at[0])

    take(SHARED, 28)
    for line in lines:
        take(line.number * PER_LINE + SENT, 31 * line.kib)
    for c in range(2):
        take(BLOCKS_SENT + c, 240)
    take(SHARED_SENT, 28)
    stored.wait()
    kept.wait()


def write_out(cache_in, shared_in, cache_out, read_out, cache, xr, rdv, sems):
    shared = pltpu.make_async_copy(shared_in, xr, sems.at[0, 4])
    shared.start()
    ways = [
        tuple(ref.at[pl.ds(k * 512, 512)] for ref in (cache_in.at[0], cache, cache_out.at[0]))
        for k in range(4)
    ]
    reads = [pltpu.make_async_copy(a, b, sems.at[0, n]) for n, (a, b, _) in enumerate(ways)]
    writes = [pltpu.make_async_copy(b, c, sems.at[1, n]) for n, (_, b, c) in enumerate(ways)]
    for copy in reads:
        copy.start()
    left8 = lax.broadcasted_iota(jnp.int32, (8, 128), 1) < HD
    turn = lambda v: pltpu.roll(v, HD, 1)
    shared.wait()
    carry = jnp.zeros((8, 128), F32)
    result = jnp.zeros((8, 128), F32)
    for t in reversed(range(8)):
        tile = xr[t]
        result = result + jnp.exp(carry) * tile
        carry = carry + turn(tile)
    result = jnp.where(left8, result, turn(result))
    for k in range(4):
        rdv[:, k * 128 : (k + 1) * 128] = jnp.where(
            left8[:1], result[2 * k : 2 * k + 1], result[2 * k + 1 : 2 * k + 2]
        )
    answered = pltpu.make_async_copy(rdv, read_out, sems.at[1, 4])
    answered.start()
    for before, after in zip(reads, writes):
        before.wait()
        after.start()
    for copy in writes:
        copy.wait()
    answered.wait()


def local(tokens, ln_gain, w_key, w_value, queries, head_shift, key_shift):
    any_ = pl.BlockSpec(memory_space=pl.ANY)
    cache, shared = pl.pallas_call(
        kernel,
        out_shape=(
            jax.ShapeDtypeStruct((1, 2048, 128), BF16),
            jax.ShapeDtypeStruct((8, 8, 128), F32),
        ),
        in_specs=[any_] * 7,
        out_specs=(any_, any_),
        scratch_shapes=[
            pltpu.VMEM((4, 128, D), BF16),
            pltpu.VMEM((512, D), BF16),
            pltpu.VMEM((2, 4, 4, 256, 256), BF16),
            pltpu.VMEM((512, 256), F32),
            pltpu.VMEM((2, 16, 64, 128), BF16),
            pltpu.VMEM((2, 16, 64, 128), BF16),
            pltpu.VMEM((2048, 128), BF16),
            pltpu.VMEM((D,), BF16),
            pltpu.VMEM((1, 512), BF16),
            pltpu.VMEM((4, 8), F32),
            pltpu.VMEM((1, 2048), F32),
            pltpu.VMEM((8, 128), F32),
            pltpu.VMEM((4096, 128), BF16),
            pltpu.SemaphoreType.DMA((14,)),
            pltpu.SemaphoreType.DMA((SEMAPHORES,)),
        ],
        compiler_params=pltpu.CompilerParams(collective_id=0, has_side_effects=True),
    )(tokens, ln_gain, w_key, w_value, queries, head_shift, key_shift)
    return pl.pallas_call(
        write_out,
        out_shape=(
            jax.ShapeDtypeStruct((1, 2048, 128), BF16),
            jax.ShapeDtypeStruct((1, 512), F32),
        ),
        in_specs=[any_] * 2,
        out_specs=(any_, any_),
        scratch_shapes=[
            pltpu.VMEM((2048, 128), BF16),
            pltpu.VMEM((8, 8, 128), F32),
            pltpu.VMEM((1, 512), F32),
            pltpu.SemaphoreType.DMA((2, 5)),
        ],
    )(cache, shared)


def solution(mesh):
    placed = (
        P("gr", "tp", "sp", None),
        P(),
        P("sp", None),
        P("sp", None),
        P(("gr", "sp"), None),
        P(),
        P(("gr", "sp"), "tp"),
    )
    return jax.shard_map(
        local,
        mesh=mesh,
        in_specs=placed,
        out_specs=(P(("gr", "sp"), "tp", None), P(("gr", "sp"), None)),
        check_vma=False,
    )
```

```python
import functools

import jax
import jax.numpy as jnp
from jax import lax
from jax.experimental import pallas as pl
from jax.experimental.pallas import tpu as pltpu
from jax.sharding import PartitionSpec as P

MESH = pl.DeviceIdType.MESH
F32, BF16 = jnp.float32, jnp.bfloat16
D, HD, KVH, GROUP = 4096, 64, 4, 8
EPS = 1e-05
SPLIT = (128, 128)
LINES, PER_LINE = 4, 8
NEAR, FAR, SECOND, PAIR, SENT, LATE = 0, 1, (2, 3, 4), 5, 6, 7
BLOCKS, BLOCKS_SENT = LINES * PER_LINE, LINES * PER_LINE + 2
SHARED, SHARED_SENT = BLOCKS + 4, BLOCKS + 5
SEMAPHORES = BLOCKS + 6
GROUPS = ((2, 3), (1, 0))


class Line:
    def __init__(self, number, c, way, rows):
        self.number, self.c, self.way, self.rows = number, c, way, rows


def kernel(
    tok_hbm, gain_hbm, wk_hbm, wv_hbm, q_hbm, hs_hbm, ks_hbm,
    cache_hbm, xr,
    tok, nrm, w, acc, kvs, kvr, cache, gain, qv, hsv, ksv, xs,
    ruler, local_sem, sems,
):
    gr, sp, tp = lax.axis_index("gr"), lax.axis_index("sp"), lax.axis_index("tp")
    x, core = tp // 2, tp % 2
    zl, y = sp // 4, sp % 4
    z = gr * 4 + zl

    def at_z(k):
        far = (z + k) % 8
        return (far // 4, (far % 4) * 4 + y, tp)

    def at_y(k):
        return (gr, zl * 4 + (y + k) % 4, tp)

    def at_sp(k):
        return (gr, (sp + k) % 16, tp)

    def at_tp(k):
        return (gr, sp, (tp + k) % 8)

    sibling = (gr, sp, x * 2 + 1 - core)

    def send(src, dst, device, sent, arrived):
        pltpu.make_async_remote_copy(
            src_ref=src,
            dst_ref=dst,
            send_sem=sems.at[sent],
            recv_sem=sems.at[arrived],
            device_id=device,
            device_id_type=MESH,
        ).start()

    def take(number, kib):
        span = ruler.at[pl.ds(0, kib * 4), :]
        pltpu.make_async_copy(span, span, sems.at[number]).wait()

    locals_ = []

    def fetch(src, dst):
        copy = pltpu.make_async_copy(src, dst, local_sem.at[len(locals_)])
        copy.start()
        locals_.append(copy)
        return copy

    barrier = pltpu.get_barrier_semaphore()
    friends = [at_z(k) for k in (1, -1, 2, -2)]
    friends += [at_y(k) for k in (1, -1, 2)]
    friends += [at_tp(k) for k in range(1, 8)]
    for friend in friends:
        pl.semaphore_signal(barrier, inc=1, device_id=friend, device_id_type=MESH)

    lines = []
    for c in range(2):
        for way in range(2):
            start = pl.multiple_of(way * SPLIT[0] + core * (SPLIT[way] // 2), 32)
            lines.append(Line(len(lines), c, way, pl.ds(start, SPLIT[way] // 2)))
            lines[-1].kib = SPLIT[way] // 4
    for line in lines:
        source = (wk_hbm, wv_hbm)[line.c].at[line.rows, :]
        line.own = fetch(source, w.at[line.c, zl, y, line.rows, :])
    got_gain = fetch(gain_hbm, gain)
    got_tok = [fetch(tok_hbm.at[s, 0], tok.at[s]) for s in range(4)]
    got_small = [fetch(q_hbm, qv), fetch(hs_hbm, hsv), fetch(ks_hbm, ksv)]

    pl.semaphore_wait(barrier, len(friends))

    every = pl.ds(0, 4)
    side = 1 - 2 * core

    def shift(line, i, j):
        mine = (y, zl) if line.way == 1 else (zl, y)
        return tuple(
            v if k is None else v if isinstance(k, int) and k == 0 else (v + k + 4) % 4
            for v, k in zip(mine, (i, j))
        )

    def pass_on(line, i, j, device, kind):
        a, b = (every if k is None else v for k, v in zip((i, j), shift(line, i, j)))
        if line.way == 1:
            a, b = b, a
        ref = w.at[line.c, a, b, line.rows, :]
        base = line.number * PER_LINE
        send(ref, ref, device, base + SENT, base + kind)

    def arrived(line, kind, pieces):
        take(line.number * PER_LINE + kind, pieces * line.kib)

    def one(line, k):
        return at_y(k) if line.way == 1 else at_z(k)

    def two(line, k):
        return at_z(k) if line.way == 1 else at_y(k)

    def offsets(along_z):
        return (2 * side if along_z else 2, 1, -1)

    def along(line, i):
        for k, kind in zip(offsets(line.way == 1), SECOND):
            pass_on(line, i, 0, two(line, k), LATE if i == 2 else kind)

    def wave0(line):
        line.own.wait()
        for k, kind in reversed(list(zip(offsets(line.way == 0), (FAR, NEAR, NEAR)))):
            pass_on(line, 0, 0, one(line, k), kind)

    def wave1(line):
        along(line, 0)

    def wave2(line):
        arrived(line, NEAR, 2)
        along(line, -1)
        along(line, 1)

    def wave3(line):
        arrived(line, FAR, 1)
        along(line, 2)
        pass_on(line, None, 0, sibling, PAIR)

    def wave4(line):
        for n, j in ((1, -1), (2, 1), (0, 2)):
            arrived(line, SECOND[n], 3)
            for i in (0, -1, 1):
                pass_on(line, i, j, sibling, PAIR)

    def wave6(line):
        arrived(line, LATE, 3)
        for j in (-1, 1, 2):
            pass_on(line, 2, j, sibling, PAIR)

    def wave5(line):
        arrived(line, PAIR, 16)

    def norm(s):
        got_tok[s].wait()

        def block(i, carry):
            for half in range(2):
                r = pl.multiple_of(i * 32 + half * 16, 16)
                rows = pl.ds(r, 16)
                tile = lambda j: tok[s, rows, j * 128 : (j + 1) * 128].astype(F32)
                sums = [tile(j) for j in range(4)]
                for j in range(4, 32):
                    sums[j % 4] = sums[j % 4] + tile(j)
                total = (sums[0] + sums[1]) + (sums[2] + sums[3])
                mean = jnp.sum(total, axis=1, keepdims=True) * (1.0 / D)
                squares = [None] * 4
                for j in range(32):
                    gap = tile(j) - mean
                    old = squares[j % 4]
                    squares[j % 4] = gap * gap if old is None else old + gap * gap
                total = (squares[0] + squares[1]) + (squares[2] + squares[3])
                var = jnp.sum(total, axis=1, keepdims=True) * (1.0 / D)
                scale = lax.rsqrt(var + EPS)
                out_rows = pl.ds(pl.multiple_of(s * 128 + r, 16), 16)
                for j in range(32):
                    cols = slice(j * 128, (j + 1) * 128)
                    value = (tile(j) - mean) * scale * gain[cols].astype(F32).reshape(1, 128)
                    nrm[out_rows, cols] = value.astype(BF16)
            return carry

        lax.fori_loop(0, 4, block, 0)

    lane = lax.broadcasted_iota(jnp.int32, (64, 128), 1)
    left = lane < HD
    left8 = left[:8]

    def turn(v):
        return pltpu.roll(v, HD, 1)

    def project(c):
        weights = w[c].reshape(D, 256)
        for group in GROUPS:
            starts = [(zl + o) % 4 for o in group]
            rows = [nrm[pl.ds(pl.multiple_of(s * 128, 128), 128), :] for s in starts]
            acc[: len(group) * 128] = jnp.dot(
                jnp.concatenate(rows, axis=0), weights, preferred_element_type=F32
            )
            for n, (o, s) in enumerate(zip(group, starts)):
                for p in range(2):
                    cols = slice(p * 128, (p + 1) * 128)
                    top = acc[n * 128 : n * 128 + 64, cols]
                    bottom = acc[n * 128 + 64 : n * 128 + 128, cols]
                    even = jnp.where(left, top, turn(bottom))
                    odd = jnp.where(left, turn(top), bottom)
                    kvs[c, s * 4 + 2 * p] = even.astype(BF16)
                    kvs[c, s * 4 + 2 * p + 1] = odd.astype(BF16)
                for k in range(4):
                    far = s * 4 + (y + k) % 4
                    if o or k:
                        device = (gr, far, tp)
                        send(kvs.at[c, far], kvr.at[c, sp], device, BLOCKS_SENT + c, BLOCKS + c)
                    else:
                        kvr[c, sp] = kvs[c, sp]

    k_lines = [line for line in lines if line.c == 0]
    v_lines = [line for line in lines if line.c == 1]

    def each(wave, some):
        for line in some:
            wave(line)

    each(wave0, k_lines)
    each(wave0, v_lines)
    each(wave1, k_lines)
    got_gain.wait()
    norm(0)
    each(wave2, k_lines)
    each(wave3, k_lines)
    each(wave1, v_lines)
    each(wave2, v_lines)
    each(wave3, v_lines)
    norm(1)
    norm(2)
    each(wave4, k_lines)
    norm(3)
    each(wave6, k_lines)
    each(wave5, k_lines)
    project(0)
    each(wave4, v_lines)
    each(wave6, v_lines)
    each(wave5, v_lines)
    project(1)

    for copy in got_small:
        copy.wait()
    row8 = lax.broadcasted_iota(jnp.int32, (8, 128), 0)
    qq = jnp.zeros((8, 128), F32)
    for g in range(GROUP):
        part = qv[:, (g // 2) * 128 : (g // 2 + 1) * 128].astype(F32)
        part = jnp.broadcast_to(part, (8, 128))
        other = turn(part)
        mine = jnp.where(left8, part, other) if g % 2 == 0 else jnp.where(left8, other, part)
        qq = jnp.where(row8 == g, mine, qq)
    q_lo = jnp.where(left8, qq, 0.0)
    q_hi = jnp.where(left8, 0.0, qq)
    stack = jnp.concatenate([q_lo, q_hi], axis=0).astype(BF16)
    hrow = lax.broadcasted_iota(jnp.int32, (4, 8), 0)
    own = jnp.sum(jnp.where(hrow == y, hsv[...], 0.0), axis=0, keepdims=True)
    eye = lax.broadcasted_iota(jnp.int32, (8, 8), 0) == lax.broadcasted_iota(jnp.int32, (8, 8), 1)
    head = jnp.sum(jnp.where(eye, jnp.broadcast_to(own, (8, 8)), 0.0), axis=1, keepdims=True)

    take(BLOCKS, 240)
    logits = lax.dot_general(
        stack, kvr[0].reshape(1024, 128), (((1,), (1,)), ((), ())), preferred_element_type=F32
    )
    tiles = []
    for m in range(8):
        cols = slice(m * 128, (m + 1) * 128)
        lo, hi = logits[:8, cols], logits[8:, cols]
        tiles.append(jnp.where(left8, lo, turn(hi)))
        tiles.append(jnp.where(left8, turn(lo), hi))
    z_all = jnp.concatenate(
        [
            t * HD ** (-0.5) + head + ksv[:, n * 128 : (n + 1) * 128]
            for n, t in enumerate(tiles)
        ],
        axis=0,
    )
    log_beta = jnp.minimum(z_all, 0.0) - jnp.log1p(jnp.exp(-jnp.abs(z_all)))
    log_keep = log_beta - z_all
    ri = lax.broadcasted_iota(jnp.int32, (128, 256), 0)
    ci = lax.broadcasted_iota(jnp.int32, (128, 256), 1)
    later = jnp.where((ci >= 128) | (ri > ci), 1.0, 0.0).astype(F32)
    sums = jnp.dot(
        log_keep, later, preferred_element_type=F32, precision=lax.Precision.HIGHEST
    )
    tail = jnp.zeros((8, 128), F32)
    weights = [None] * 16
    for n in reversed(range(16)):
        rows = slice(n * 8, (n + 1) * 8)
        weights[n] = jnp.exp(log_beta[rows] + (sums[rows, :128] + tail))
        tail = tail + sums[rows, 128:]
    w_lo = [jnp.where(left8, weights[2 * m], turn(weights[2 * m + 1])) for m in range(8)]
    w_hi = [jnp.where(left8, turn(weights[2 * m]), weights[2 * m + 1]) for m in range(8)]
    wstack = jnp.concatenate(
        [jnp.concatenate(w_lo, axis=1), jnp.concatenate(w_hi, axis=1)], axis=0
    ).astype(BF16)

    take(BLOCKS + 1, 240)
    out = jnp.dot(wstack, kvr[1].reshape(1024, 128), preferred_element_type=F32)
    section = out[:8] + turn(out[8:])
    message = jnp.where(left8, section, tail)
    xs[...] = message
    kept = fetch(xs, xr.at[tp])
    for k in range(1, 8):
        send(xs, xr.at[tp], at_tp(k), SHARED_SENT, SHARED)

    def assemble(j, carry):
        keys = kvr[0, j].astype(F32)
        values = kvr[1, j].astype(F32)
        first = pl.multiple_of(j * 128, 64)
        second = pl.multiple_of(j * 128 + 64, 64)
        cache[pl.ds(first, 64), :] = jnp.where(left, keys, turn(values)).astype(BF16)
        cache[pl.ds(second, 64), :] = jnp.where(left, turn(keys), values).astype(BF16)
        return carry

    lax.fori_loop(0, 16, assemble, 0)
    stored = fetch(cache, cache_hbm.at[0])

    take(SHARED, 28)
    for line in lines:
        take(line.number * PER_LINE + SENT, 31 * line.kib)
    for c in range(2):
        take(BLOCKS_SENT + c, 240)
    take(SHARED_SENT, 28)
    stored.wait()
    kept.wait()


def write_out(cache_in, shared_in, cache_out, read_out, cache, xr, rdv, sems):
    shared = pltpu.make_async_copy(shared_in, xr, sems.at[0, 4])
    shared.start()
    ways = [
        tuple(ref.at[pl.ds(k * 512, 512)] for ref in (cache_in.at[0], cache, cache_out.at[0]))
        for k in range(4)
    ]
    reads = [pltpu.make_async_copy(a, b, sems.at[0, n]) for n, (a, b, _) in enumerate(ways)]
    writes = [pltpu.make_async_copy(b, c, sems.at[1, n]) for n, (_, b, c) in enumerate(ways)]
    for copy in reads:
        copy.start()
    left8 = lax.broadcasted_iota(jnp.int32, (8, 128), 1) < HD
    turn = lambda v: pltpu.roll(v, HD, 1)
    shared.wait()
    carry = jnp.zeros((8, 128), F32)
    result = jnp.zeros((8, 128), F32)
    for t in reversed(range(8)):
        tile = xr[t]
        result = result + jnp.exp(carry) * tile
        carry = carry + turn(tile)
    result = jnp.where(left8, result, turn(result))
    for k in range(4):
        rdv[:, k * 128 : (k + 1) * 128] = jnp.where(
            left8[:1], result[2 * k : 2 * k + 1], result[2 * k + 1 : 2 * k + 2]
        )
    answered = pltpu.make_async_copy(rdv, read_out, sems.at[1, 4])
    answered.start()
    for before, after in zip(reads, writes):
        before.wait()
        after.start()
    for copy in writes:
        copy.wait()
    answered.wait()


def local(tokens, ln_gain, w_key, w_value, queries, head_shift, key_shift):
    any_ = pl.BlockSpec(memory_space=pl.ANY)
    cache, shared = pl.pallas_call(
        kernel,
        out_shape=(
            jax.ShapeDtypeStruct((1, 2048, 128), BF16),
            jax.ShapeDtypeStruct((8, 8, 128), F32),
        ),
        in_specs=[any_] * 7,
        out_specs=(any_, any_),
        scratch_shapes=[
            pltpu.VMEM((4, 128, D), BF16),
            pltpu.VMEM((512, D), BF16),
            pltpu.VMEM((2, 4, 4, 256, 256), BF16),
            pltpu.VMEM((512, 256), F32),
            pltpu.VMEM((2, 16, 64, 128), BF16),
            pltpu.VMEM((2, 16, 64, 128), BF16),
            pltpu.VMEM((2048, 128), BF16),
            pltpu.VMEM((D,), BF16),
            pltpu.VMEM((1, 512), BF16),
            pltpu.VMEM((4, 8), F32),
            pltpu.VMEM((1, 2048), F32),
            pltpu.VMEM((8, 128), F32),
            pltpu.VMEM((4096, 128), BF16),
            pltpu.SemaphoreType.DMA((14,)),
            pltpu.SemaphoreType.DMA((SEMAPHORES,)),
        ],
        compiler_params=pltpu.CompilerParams(collective_id=0, has_side_effects=True),
    )(tokens, ln_gain, w_key, w_value, queries, head_shift, key_shift)
    return pl.pallas_call(
        write_out,
        out_shape=(
            jax.ShapeDtypeStruct((1, 2048, 128), BF16),
            jax.ShapeDtypeStruct((1, 512), F32),
        ),
        in_specs=[any_] * 2,
        out_specs=(any_, any_),
        scratch_shapes=[
            pltpu.VMEM((2048, 128), BF16),
            pltpu.VMEM((8, 8, 128), F32),
            pltpu.VMEM((1, 512), F32),
            pltpu.SemaphoreType.DMA((2, 5)),
        ],
    )(cache, shared)


def solution(mesh):
    placed = (
        P("gr", "tp", "sp", None),
        P(),
        P("sp", None),
        P("sp", None),
        P(("gr", "sp"), None),
        P(),
        P(("gr", "sp"), "tp"),
    )
    return jax.shard_map(
        local,
        mesh=mesh,
        in_specs=placed,
        out_specs=(P(("gr", "sp"), "tp", None), P(("gr", "sp"), None)),
        check_vma=False,
    )
```
